32 devices in a mesh: grp: 2 (over y), kv: 4 (over z), tp: 4 (over x, core).
Axes of the slice: x: 2, y: 2, z: 4, core: 2. Of those that a mesh axis runs over, the one named last changes fastest.
Arguments:
- tokens: bfloat16 [64, 4096], P('grp', ('kv', 'tp')), parts along dimension 0, may hold values from -12 to 12
- gain_in: float32 [4096], P('kv'), may hold values from 0.1 to 1.9
- w_query: bfloat16 [4096, 1024], P('kv', 'tp'), may hold values from -0.09375 to 0.09375
- w_key: bfloat16 [4096, 1024], P('kv', 'tp'), may hold values from -0.09375 to 0.09375
- w_value: bfloat16 [4096, 2048], P('kv', 'tp'), may hold values from -0.09375 to 0.09375
- w_outgate: bfloat16 [4096, 2048], P('kv', 'tp'), may hold values from -0.09375 to 0.09375
- w_input_gate: bfloat16 [4096, 16], P('kv'), may hold values from -0.09375 to 0.09375
- w_forget_gate: bfloat16 [4096, 16], P('kv'), may hold values from -0.09375 to 0.09375
- bias_input: float32 [16], replicated, may hold values from -1 to 1
- bias_forget: float32 [16], replicated, may hold values from -1 to 4
- cell_state: float32 [64, 16, 64, 128], P(('grp', 'kv'), 'tp'), parts along dimension 0, may hold values from -6 to 6
- norm_state: float32 [64, 16, 64], P(('grp', 'kv'), 'tp'), parts along dimension 0, may hold values from -18 to 18
- max_state: float32 [64, 16], P(('grp', 'kv'), 'tp'), parts along dimension 0, may hold values from -1 to 2
- w_proj: bfloat16 [2048, 4096], P('tp', 'kv'), may hold values from -0.125 to 0.125
- gain_mid: float32 [4096], P('kv'), may hold values from 0.1 to 1.9
- w_up: bfloat16 [4096, 16384], P('kv', 'tp'), may hold values from -0.09375 to 0.09375
- w_down: bfloat16 [16384, 4096], P('tp', 'kv'), may hold values from -0.046875 to 0.046875
Outputs:
- mixed: bfloat16 [64, 4096], P('grp', ('kv', 'tp')), parts along dimension 0
- cell_new: float32 [64, 16, 64, 128], P(('grp', 'kv'), 'tp'), parts along dimension 0
- norm_new: float32 [64, 16, 64], P(('grp', 'kv'), 'tp'), parts along dimension 0
- max_new: float32 [64, 16], P(('grp', 'kv'), 'tp'), parts along dimension 0
The draws below stay inside these ranges and needn't reach their ends.
There are 2 independent parts, one for each index of `grp`. The reference program is written for one: setup_inputs(seed, part) draws one part's arguments, and reference() takes and returns one part's arrays. A program takes and returns all parts, laid end to end along the dimension named above; an argument that names none is the same for every part. Nothing has to cross between parts.
All inputs are finite; a program needn't handle non-finite values.
Results may differ from the reference program's by a relative error of at most 0.015.
Values may be sent and summed in bfloat16 or wider, within the bound.
A program may use at most 64 MiB of HBM per device.

```python
import math
import jax
import jax.numpy as jnp
from jax import lax

D = 4096
NH = 16
DQK = 64
DV = 128
FF = 16384
BATCH = 32


def draw_tokens(key, part):
    key_scale = jax.random.fold_in(key, 11)
    key_base = jax.random.fold_in(key, 12)
    scales = jnp.exp(jax.random.uniform(key_scale, (16,), jnp.float32, math.log(0.3), math.log(3.0)))
    base = jnp.clip(jax.random.normal(key_base, (BATCH, D), jnp.float32), -4.0, 4.0)
    return (base * jnp.repeat(scales, D // 16)[None, :]).astype(jnp.bfloat16)


def block_levels(key, dims, pieces, smallest, top_value):
    level = 1.0
    for position, parts in pieces:
        draws = jax.random.uniform(jax.random.fold_in(jax.random.fold_in(key, 6), position), (parts,), jnp.float32, smallest / len(pieces), top_value / len(pieces))
        level = level * jnp.repeat(jnp.exp(draws), dims[position] // parts).reshape((-1,) + (1,) * (len(dims) - 1 - position))
    return level


def scatter_about(rng, extent, spread, limit, split=(), dtype=jnp.bfloat16):
    gain = block_levels(rng, extent, split, -0.22, 0.18) if split else 1.0
    array = jax.random.normal(rng, extent, jnp.float32) * spread * gain
    return jnp.minimum(jnp.maximum(array, -limit), limit).astype(dtype)


def setup_inputs(seed: int = 0, part: int = 0) -> dict:
    streams_of = jax.random.split(jax.random.key(seed), 18)
    own_keys = jax.random.split(jax.random.fold_in(streams_of[17], part), 18)
    return {
        "tokens": draw_tokens(jax.random.fold_in(jax.random.fold_in(streams_of[17], part), 71), part),
        "gain_in": jnp.clip(1.0 + 0.18 * jax.random.normal(streams_of[1], (D,), jnp.float32), 0.1, 1.9),
        "w_query": scatter_about(streams_of[2], (D, NH * DQK), D ** -0.5, 0.09375, ((0, 4), (1, 4))),
        "w_key": scatter_about(streams_of[3], (D, NH * DQK), D ** -0.5, 0.09375, ((0, 4), (1, 4))),
        "w_value": scatter_about(streams_of[4], (D, NH * DV), D ** -0.5, 0.09375, ((0, 4), (1, 4))),
        "w_outgate": scatter_about(streams_of[5], (D, NH * DV), D ** -0.5, 0.09375, ((0, 4), (1, 4))),
        "w_input_gate": scatter_about(streams_of[6], (D, NH), D ** -0.5, 0.09375, ((0, 4),)),
        "w_forget_gate": scatter_about(streams_of[7], (D, NH), D ** -0.5, 0.09375, ((0, 4),)),
        "bias_input": jnp.clip(jax.random.uniform(streams_of[8], (NH,), jnp.float32, -1.0, 1.0), -1.0, 1.0),
        "bias_forget": jnp.clip(jax.random.uniform(streams_of[9], (NH,), jnp.float32, -1.0, 4.0), -1.0, 4.0),
        "cell_state": scatter_about(own_keys[10], (BATCH, NH, DQK, DV), 1.0, 6.0, ((0, 4), (1, 4)), jnp.float32),
        "norm_state": scatter_about(own_keys[11], (BATCH, NH, DQK), 3.0, 18.0, ((0, 4), (1, 4)), jnp.float32),
        "max_state": jnp.clip(-1.0 + 3.0 * jax.random.uniform(own_keys[12], (BATCH, NH), jnp.float32) ** block_levels(own_keys[12], (BATCH, NH), ((0, 4), (1, 4)), -0.2, 0.2), -1.0, 2.0),
        "w_proj": scatter_about(streams_of[13], (NH * DV, D), (NH * DV) ** -0.5, 0.125, ((0, 4), (1, 4))),
        "gain_mid": jnp.clip(1.0 + 0.18 * jax.random.normal(streams_of[14], (D,), jnp.float32), 0.1, 1.9),
        "w_up": scatter_about(streams_of[15], (D, FF), D ** -0.5, 0.09375, ((0, 4), (1, 4))),
        "w_down": scatter_about(streams_of[16], (FF, D), FF ** -0.5, 0.046875, ((0, 4), (1, 4))),
    }


EPSILON = 1e-06

def memory_step(query, keys, values, outgate, log_input, log_forget, cell_state, norm_state, max_state):
    max_new = jnp.maximum(log_forget + max_state, log_input)
    keep = jnp.exp(log_forget + max_state - max_new)
    write = jnp.exp(log_input - max_new)
    cell_new = keep[..., None, None] * cell_state + (write[..., None] * keys)[..., :, None] * values[..., None, :]
    norm_new = keep[..., None] * norm_state + write[..., None] * keys
    numer = jnp.einsum('shk,shkv->shv', query, cell_new, precision=lax.Precision.HIGHEST)
    denom = jnp.maximum(jnp.abs(lax.optimization_barrier(jnp.sum(query * norm_new, axis=-1))), jnp.exp(-max_new))
    heads = (jax.nn.sigmoid(outgate) * numer / denom[..., None]).astype(jnp.bfloat16)
    return (heads, cell_new, norm_new, max_new)

def reference(tokens, gain_in, w_query, w_key, w_value, w_outgate, w_input_gate, w_forget_gate, bias_input, bias_forget, cell_state, norm_state, max_state, w_proj, gain_mid, w_up, w_down):
    rows = tokens.shape[0]
    widef = tokens.astype(jnp.float32)
    scale_in = lax.rsqrt(lax.optimization_barrier(jnp.sum(widef * widef, axis=1)) / D + EPSILON)
    normed = (widef * gain_in).astype(jnp.bfloat16)

    def project(weight):
        return jnp.dot(normed, weight, preferred_element_type=jnp.float32) * scale_in[:, None]
    query = project(w_query).reshape(rows, NH, DQK) * DQK ** (-0.5)
    keys = project(w_key).reshape(rows, NH, DQK)
    values = project(w_value).reshape(rows, NH, DV)
    outgate = project(w_outgate).reshape(rows, NH, DV)
    log_input = project(w_input_gate) + bias_input
    log_forget = jax.nn.log_sigmoid(project(w_forget_gate) + bias_forget)
    heads, cell_new, norm_new, max_new = memory_step(query, keys, values, outgate, log_input, log_forget, cell_state, norm_state, max_state)
    branch = jnp.dot(heads.reshape(rows, NH * DV), w_proj, preferred_element_type=jnp.float32)
    middle = (widef + branch).astype(jnp.bfloat16)
    midf = middle.astype(jnp.float32)
    scale_mid = lax.rsqrt(lax.optimization_barrier(jnp.sum(midf * midf, axis=1)) / D + EPSILON)
    normed_mid = (midf * gain_mid).astype(jnp.bfloat16)
    upward = jnp.dot(normed_mid, w_up, preferred_element_type=jnp.float32) * scale_mid[:, None]
    hidden = jnp.square(jax.nn.relu(upward)).astype(jnp.bfloat16)
    down = jnp.dot(hidden, w_down, preferred_element_type=jnp.float32)
    mixed = (midf + down).astype(jnp.bfloat16)
    return (mixed, cell_new, norm_new, max_new)
```

```python
import functools

import jax
import jax.numpy as jnp
from jax import lax
from jax.experimental import pallas as pl
from jax.experimental.pallas import tpu as pltpu
from jax.sharding import PartitionSpec as P

MESH = pl.DeviceIdType.MESH
BF16 = jnp.bfloat16
F32 = jnp.float32

EPSILON = 1e-06


def memory_step(
    query, keys, values, outgate, log_input, log_forget, cell_state, norm_state, max_state
):
    max_new = jnp.maximum(log_forget + max_state, log_input)
    keep = jnp.exp(log_forget + max_state - max_new)
    write = jnp.exp(log_input - max_new)
    cell_new = (
        keep[..., None, None] * cell_state
        + (write[..., None] * keys)[..., :, None] * values[..., None, :]
    )
    norm_new = keep[..., None] * norm_state + write[..., None] * keys
    numer = jnp.einsum("shk,shkv->shv", query, cell_new, precision=lax.Precision.HIGHEST)
    denom = jnp.maximum(jnp.abs(jnp.sum(query * norm_new, axis=-1)), jnp.exp(-max_new))
    heads = (jax.nn.sigmoid(outgate) * numer / denom[..., None]).astype(jnp.bfloat16)
    return (heads, cell_new, norm_new, max_new)


def matmul(left, right):
    return jnp.dot(left, right, preferred_element_type=jnp.float32)


def plain_on_device(
    tokens,
    gain_in,
    w_query,
    w_key,
    w_value,
    w_outgate,
    w_input_gate,
    w_forget_gate,
    bias_input,
    bias_forget,
    cell_state,
    norm_state,
    max_state,
    w_proj,
    gain_mid,
    w_up,
    w_down,
):
    seq_local, head_count = (cell_state.shape[0], cell_state.shape[1])
    key_dim, value_dim = (cell_state.shape[2], cell_state.shape[3])
    head_start = lax.axis_index("tp") * head_count
    column_width = tokens.shape[1]
    D = gain_in.shape[0] * lax.axis_size("kv")
    gathered = lax.all_gather(tokens, "tp", axis=1, tiled=True)
    widef = gathered.astype(jnp.float32)
    part_squares = jnp.sum(widef * widef, axis=1)
    normed = (widef * gain_in).astype(jnp.bfloat16)
    gate_input = lax.dynamic_slice_in_dim(w_input_gate, head_start, head_count, 1)
    gate_forget = lax.dynamic_slice_in_dim(w_forget_gate, head_start, head_count, 1)
    terms = jnp.concatenate(
        [
            matmul(normed, w_query),
            matmul(normed, w_key),
            matmul(normed, w_value),
            matmul(normed, w_outgate),
            matmul(normed, gate_input),
            matmul(normed, gate_forget),
        ],
        axis=1,
    )
    total_squares = lax.psum(part_squares, "kv")
    own_terms = lax.psum_scatter(terms, "kv", scatter_dimension=0, tiled=True)
    row_squares = lax.dynamic_slice_in_dim(
        total_squares, lax.axis_index("kv") * seq_local, seq_local, 0
    )
    own_terms = own_terms * lax.rsqrt(row_squares / D + EPSILON)[:, None]
    width_qk = head_count * key_dim
    width_v = head_count * value_dim
    query = own_terms[:, :width_qk].reshape(seq_local, head_count, key_dim) * key_dim ** (-0.5)
    keys = own_terms[:, width_qk : 2 * width_qk].reshape(seq_local, head_count, key_dim)
    offset = 2 * width_qk
    values = own_terms[:, offset : offset + width_v].reshape(seq_local, head_count, value_dim)
    offset = offset + width_v
    outgate = own_terms[:, offset : offset + width_v].reshape(seq_local, head_count, value_dim)
    offset = offset + width_v
    log_input = own_terms[:, offset : offset + head_count] + lax.dynamic_slice_in_dim(
        bias_input, head_start, head_count, 0
    )
    offset = offset + head_count
    log_forget = jax.nn.log_sigmoid(
        own_terms[:, offset : offset + head_count]
        + lax.dynamic_slice_in_dim(bias_forget, head_start, head_count, 0)
    )
    heads, cell_new, norm_new, max_new = memory_step(
        query, keys, values, outgate, log_input, log_forget, cell_state, norm_state, max_state
    )
    branch_part = matmul(
        lax.all_gather(heads.reshape(seq_local, width_v), "kv", axis=0, tiled=True), w_proj
    )
    branch = lax.psum(branch_part, "tp")
    middle = (widef + branch).astype(jnp.bfloat16)
    midf = middle.astype(jnp.float32)
    mid_squares = jnp.sum(midf * midf, axis=1)
    normed_mid = (midf * gain_mid).astype(jnp.bfloat16)
    up_part = matmul(normed_mid, w_up)
    up_rows, square_rows = (
        lax.psum_scatter(up_part, "kv", scatter_dimension=0, tiled=True),
        lax.psum_scatter(mid_squares, "kv", scatter_dimension=0, tiled=True),
    )
    upward = up_rows * lax.rsqrt(square_rows / D + EPSILON)[:, None]
    hidden = jnp.square(jax.nn.relu(upward)).astype(jnp.bfloat16)
    down_part = matmul(lax.all_gather(hidden, "kv", axis=0, tiled=True), w_down)
    own_down = lax.psum_scatter(
        down_part.astype(jnp.bfloat16), "tp", scatter_dimension=1, tiled=True
    ).astype(jnp.float32)
    residual = lax.dynamic_slice_in_dim(midf, lax.axis_index("tp") * column_width, column_width, 1)
    mixed = (residual + own_down).astype(jnp.bfloat16)
    return (mixed, cell_new, norm_new, max_new)


class Exchange:
    def __init__(self, sems):
        self.send_sem, self.recv_sem = sems
        self.used = 0
        self.started = []

    def copy(self, axis, target, src, dst):
        index = self.used
        self.used += 1
        one = pltpu.make_async_remote_copy(
            src_ref=src,
            dst_ref=dst,
            send_sem=self.send_sem.at[index],
            recv_sem=self.recv_sem.at[index],
            device_id={axis: target},
            device_id_type=MESH,
        )
        one.start()
        self.started.append(one)
        return one


def count_copies(kv, tp, subs):
    return 3 * (tp - 1) + 4 * (kv - 1) + 2 * subs * (kv - 1)


def layer_kernel(
    kv,
    tp,
    subs,
    tokens,
    gain_in,
    w_query,
    w_key,
    w_value,
    w_outgate,
    w_input_gate,
    w_forget_gate,
    bias_input,
    bias_forget,
    cell_state,
    norm_state,
    max_state,
    w_proj,
    gain_mid,
    w_up,
    w_down,
    mixed,
    cell_new,
    norm_new,
    max_new,
    tok,
    gain1,
    wqkv,
    wgi,
    wgf,
    bi,
    bf,
    cell,
    norm,
    mstate,
    wproj,
    gain2,
    wup,
    wdown,
    out_v,
    cell_o,
    norm_o,
    max_o,
    terms,
    b_send,
    b_recv,
    g_send,
    g_recv,
    numer,
    h_all,
    e_all,
    sq_all,
    mid,
    nmid,
    f_own,
    f_send,
    f_recv,
    hid,
    down,
    d_send,
    d_recv,
    in_sem,
    out_sem,
    send_sem,
    recv_sem,
):
    k_me, t_me = lax.axis_index("kv"), lax.axis_index("tp")
    link = Exchange((send_sem, recv_sem))
    rows, width = tok.shape[1], tok.shape[2]
    own_rows, n_heads, key_dim, value_dim = cell.shape
    wide = tp * width
    total_width = kv * wide
    w_qk, w_v = n_heads * key_dim, n_heads * value_dim
    half = f_own.shape[2]
    block = subs * half

    loads = []

    def load(src, dst):
        one = pltpu.make_async_copy(src, dst, in_sem.at[len(loads)])
        one.start()
        loads.append(one)
        return one

    l_tok = load(tokens, tok.at[t_me])
    l_gain = load(gain_in, gain1)
    l_q = load(w_query, wqkv.at[:, 0:w_qk])
    l_k = load(w_key, wqkv.at[:, w_qk : 2 * w_qk])
    l_v = load(w_value, wqkv.at[:, 2 * w_qk : 2 * w_qk + w_v])
    l_o = load(w_outgate, wqkv.at[:, 2 * w_qk + w_v : 2 * w_qk + 2 * w_v])
    l_gates = [load(w_input_gate, wgi), load(w_forget_gate, wgf)]
    l_small = [
        load(bias_input, bi),
        load(bias_forget, bf),
        load(norm_state, norm),
        load(max_state, mstate),
    ]
    l_cell = load(cell_state, cell)
    l_proj = load(w_proj, wproj)
    l_gain2 = load(gain_mid, gain2)
    l_up = load(w_up, wup)
    l_down = [
        load(w_down.at[pl.ds(i * block, block)], wdown.at[pl.ds(i * block, block)])
        for i in range(kv)
    ]

    barrier = pltpu.get_barrier_semaphore()
    k_peers = [lax.rem(k_me + o, kv) for o in range(1, kv)]
    t_peers = [lax.rem(t_me + o, tp) for o in range(1, tp)]
    for peer in t_peers:
        pl.semaphore_signal(barrier, inc=1, device_id={"tp": peer}, device_id_type=MESH)
    for peer in k_peers:
        pl.semaphore_signal(barrier, inc=1, device_id={"kv": peer}, device_id_type=MESH)
    g_send[...] = jnp.zeros_like(g_send)
    l_tok.wait()
    pl.semaphore_wait(barrier, kv + tp - 2)

    a_copies = [link.copy("tp", p, tok.at[t_me], tok.at[t_me]) for p in t_peers]
    l_gain.wait()
    for one in a_copies:
        one.wait_recv()
    wide_f = jnp.concatenate([tok[i] for i in range(tp)], axis=1).astype(F32)
    squares = jnp.sum(wide_f * wide_f, axis=1, keepdims=True)
    normed = (wide_f * gain1[...]).astype(BF16)

    for one in l_gates:
        one.wait()
    n_gates = wgi.shape[1]
    shape_g = (kv, own_rows, n_gates)
    g_send[:, :, 0:n_gates] = matmul(normed, wgi[...]).reshape(shape_g)
    g_send[:, :, 128 : 128 + n_gates] = matmul(normed, wgf[...]).reshape(shape_g)
    g_send[:, :, 256:384] = jnp.broadcast_to(squares, (rows, 128)).reshape(kv, own_rows, 128)
    g_copies = [
        link.copy("kv", p, g_send.at[p], g_recv.at[o]) for o, p in enumerate(k_peers)
    ]
    for one in (l_q, l_k, l_v, l_o):
        one.wait()
    tile = 256

    def project(i, carry):
        cols = pl.ds(pl.multiple_of(i * tile, tile), tile)
        part = matmul(normed, wqkv[:, cols]).reshape(kv, own_rows, tile)
        terms[:, :, cols] = part
        b_send[:, :, cols] = part.astype(BF16)
        return carry

    lax.fori_loop(0, wqkv.shape[1] // tile, project, 0)
    b_copies = [
        link.copy("kv", p, b_send.at[p], b_recv.at[o]) for o, p in enumerate(k_peers)
    ]

    for one in l_small:
        one.wait()
    l_cell.wait()
    for one in g_copies:
        one.wait_recv()
    gates = g_send[k_me]
    for o in range(kv - 1):
        gates = gates + g_recv[o]
    scale = lax.rsqrt(gates[:, 256:257] / total_width + EPSILON)
    log_i = gates[:, 0:n_gates] * scale + bi[...]
    raw_f = gates[:, 128 : 128 + n_gates] * scale + bf[...]
    log_f = jnp.minimum(raw_f, 0.0) - jnp.log1p(jnp.exp(-jnp.abs(raw_f)))
    gate_lane = lax.broadcasted_iota(jnp.int32, (own_rows, n_gates), 1)
    keep, write, floor = [], [], []
    for h in range(n_heads):
        pick = gate_lane == t_me * n_heads + h
        li = jnp.sum(jnp.where(pick, log_i, 0.0), axis=1, keepdims=True)
        lf = jnp.sum(jnp.where(pick, log_f, 0.0), axis=1, keepdims=True)
        old = mstate[:, h : h + 1]
        new = jnp.maximum(lf + old, li)
        max_o[:, h : h + 1] = new
        keep.append(jnp.exp(lf + old - new))
        write.append(jnp.exp(li - new))
        floor.append(jnp.exp(-new))
    outs = []

    def store(src, dst):
        one = pltpu.make_async_copy(src, dst, out_sem.at[len(outs)])
        one.start()
        outs.append(one)

    store(max_o, max_new)
    for one in b_copies:
        one.wait_recv()
    own = terms[k_me]
    for o in range(kv - 1):
        own = own + b_recv[o].astype(F32)
    own = own * scale
    query = own[:, 0:w_qk] * key_dim ** (-0.5)
    keys = own[:, w_qk : 2 * w_qk]
    values = own[:, 2 * w_qk : 2 * w_qk + w_v]
    outgate = own[:, 2 * w_qk + w_v : 2 * w_qk + 2 * w_v]
    qk_head = lax.broadcasted_iota(jnp.int32, (own_rows, w_qk), 1) // key_dim
    spread = jnp.broadcast_to(write[0], (own_rows, w_qk))
    for h in range(1, n_heads):
        spread = jnp.where(qk_head == h, write[h], spread)
    wkeys = keys * spread
    pad = jnp.zeros((128 - 2 * own_rows, w_qk), F32)
    turned = jnp.concatenate([wkeys, query, pad], axis=0).T
    denom = []
    for h in range(n_heads):
        part = slice(h * key_dim, (h + 1) * key_dim)
        fresh = keep[h] * norm[:, h, :] + wkeys[:, part]
        norm_o[:, h, :] = fresh
        dot = jnp.sum(query[:, part] * fresh, axis=1, keepdims=True)
        denom.append(
            jnp.broadcast_to(jnp.maximum(jnp.abs(dot), floor[h]), (own_rows, value_dim))
        )
    store(norm_o, norm_new)
    for h in range(n_heads):
        part = slice(h * key_dim, (h + 1) * key_dim)
        vals = slice(h * value_dim, (h + 1) * value_dim)
        for s in range(own_rows):
            fresh = (
                keep[h][s : s + 1, :] * cell[s, h]
                + turned[part, s : s + 1] * values[s : s + 1, vals]
            )
            cell_o[s, h] = fresh
            q_col = turned[part, own_rows + s : own_rows + s + 1]
            numer[s : s + 1, vals] = jnp.sum(q_col * fresh, axis=0, keepdims=True)
    heads = jax.nn.sigmoid(outgate) * numer[...] / jnp.concatenate(denom, axis=1)
    h_all[k_me] = heads.astype(BF16)
    h_copies = [link.copy("kv", p, h_all.at[k_me], h_all.at[k_me]) for p in k_peers]
    store(cell_o, cell_new)
    l_proj.wait()
    for one in h_copies:
        one.wait_recv()
    all_heads = jnp.concatenate([h_all[i].astype(F32) for i in range(kv)], axis=0)

    e_all[t_me] = matmul(all_heads.astype(BF16), wproj[...]).astype(BF16)
    e_copies = [link.copy("tp", p, e_all.at[t_me], e_all.at[t_me]) for p in t_peers]
    l_gain2.wait()
    for one in e_copies:
        one.wait_recv()
    branch = e_all[0].astype(F32)
    for i in range(1, tp):
        branch = branch + e_all[i].astype(F32)
    wide_f = jnp.concatenate([tok[i] for i in range(tp)], axis=1).astype(F32)
    middle = (wide_f + branch).astype(BF16).astype(F32)
    for i in range(tp):
        mid[i] = middle[:, i * width : (i + 1) * width]
    sq_all[k_me] = jnp.broadcast_to(jnp.sum(middle * middle, axis=1, keepdims=True), (rows, 128))
    s_copies = [link.copy("kv", p, sq_all.at[k_me], sq_all.at[k_me]) for p in k_peers]
    nmid[...] = (middle * gain2[...]).astype(BF16)

    l_up.wait()
    f_copies = {}
    for sub in range(subs):
        for o in list(range(1, kv)) + [0]:
            peer = lax.rem(k_me + o, kv)
            first = peer * block + sub * half

            def raise_tile(i, carry, first=first, o=o, sub=sub):
                cols = pl.ds(pl.multiple_of(first + i * tile, tile), tile)
                here = pl.ds(pl.multiple_of(i * tile, tile), tile)
                part = matmul(nmid[...], wup[:, cols])
                if o:
                    f_send[o - 1, sub, :, here] = part.astype(BF16)
                else:
                    f_own[sub, :, here] = part
                return carry

            lax.fori_loop(0, half // tile, raise_tile, 0)
            if o:
                f_copies[o, sub] = link.copy(
                    "kv", peer, f_send.at[o - 1, sub], f_recv.at[o - 1, sub]
                )
    for one in s_copies:
        one.wait_recv()
    row_sum = sq_all[0, :, 0:1]
    for i in range(1, kv):
        row_sum = row_sum + sq_all[i, :, 0:1]
    scale_mid = lax.rsqrt(row_sum / total_width + EPSILON)
    g2_copies = {}
    for sub in range(subs):
        upward = f_own[sub]
        for o in range(1, kv):
            f_copies[o, sub].wait_recv()
            upward = upward + f_recv[o - 1, sub].astype(F32)
        hid[k_me, sub] = jnp.square(jnp.maximum(upward * scale_mid, 0.0)).astype(BF16)
        for o in range(1, kv):
            g2_copies[o, sub] = link.copy(
                "kv", k_peers[o - 1], hid.at[k_me, sub], hid.at[k_me, sub]
            )

    for one in l_down:
        one.wait()
    for o in range(kv):
        source = lax.rem(k_me + kv - o, kv)
        for sub in range(subs):
            if o:
                g2_copies[o, sub].wait_recv()
            deep = pl.ds(pl.multiple_of(source * block + sub * half, half), half)

            def lower_tile(i, carry, source=source, sub=sub, deep=deep, o=o):
                cols = pl.ds(pl.multiple_of(i * tile, tile), tile)
                part = matmul(hid[source, sub], wdown[deep, cols])
                if o or sub:
                    part = part + down[:, cols]
                down[:, cols] = part
                return carry

            lax.fori_loop(0, wide // tile, lower_tile, 0)
    for i in range(tp):
        d_send[i] = down[:, i * width : (i + 1) * width].astype(BF16)
    d_copies = [
        link.copy("tp", p, d_send.at[p], d_recv.at[o]) for o, p in enumerate(t_peers)
    ]
    lower = d_send[t_me].astype(F32)
    for o, one in enumerate(d_copies):
        one.wait_recv()
        lower = lower + d_recv[o].astype(F32)
    out_v[...] = (mid[t_me] + lower).astype(BF16)
    store(out_v, mixed)
    for one in link.started:
        one.wait_send()
    for one in outs:
        one.wait()


def fused_on_device(kv, tp, *args):
    (tokens, gain_in, w_query, w_key, w_value, w_outgate, w_input_gate, w_forget_gate) = args[:8]
    (bias_input, bias_forget, cell_state, norm_state, max_state) = args[8:13]
    (w_proj, gain_mid, w_up, w_down) = args[13:]
    rows, width = tokens.shape
    own_rows = cell_state.shape[0]
    wide = w_query.shape[0]
    n_qkv = w_query.shape[1] + w_key.shape[1] + w_value.shape[1] + w_outgate.shape[1]
    hidden = w_up.shape[1]
    subs = 2
    half = hidden // (kv * subs)
    w_v = w_value.shape[1]
    operands = (
        tokens,
        gain_in.reshape(1, -1),
        w_query,
        w_key,
        w_value,
        w_outgate,
        w_input_gate,
        w_forget_gate,
        bias_input.reshape(1, -1),
        bias_forget.reshape(1, -1),
        cell_state,
        norm_state,
        max_state,
        w_proj,
        gain_mid.reshape(1, -1),
        w_up,
        w_down,
    )
    n_copies = count_copies(kv, tp, subs)
    vm = pltpu.VMEM
    scratch = [
        vm((tp, rows, width), BF16),
        vm((1, wide), F32),
        vm((wide, n_qkv), BF16),
        vm(w_input_gate.shape, BF16),
        vm(w_forget_gate.shape, BF16),
        vm((1, bias_input.shape[0]), F32),
        vm((1, bias_forget.shape[0]), F32),
        vm(cell_state.shape, F32),
        vm(norm_state.shape, F32),
        vm(max_state.shape, F32),
        vm(w_proj.shape, BF16),
        vm((1, wide), F32),
        vm(w_up.shape, BF16),
        vm(w_down.shape, BF16),
        vm((rows, width), BF16),
        vm(cell_state.shape, F32),
        vm(norm_state.shape, F32),
        vm(max_state.shape, F32),
        vm((kv, own_rows, n_qkv), F32),
        vm((kv, own_rows, n_qkv), BF16),
        vm((kv - 1, own_rows, n_qkv), BF16),
        vm((kv, own_rows, 384), F32),
        vm((kv - 1, own_rows, 384), F32),
        vm((own_rows, w_v), F32),
        vm((kv, own_rows, w_v), BF16),
        vm((tp, rows, wide), BF16),
        vm((kv, rows, 128), F32),
        vm((tp, rows, width), F32),
        vm((rows, wide), BF16),
        vm((subs, rows, half), F32),
        vm((kv - 1, subs, rows, half), BF16),
        vm((kv - 1, subs, rows, half), BF16),
        vm((kv, subs, rows, half), BF16),
        vm((rows, wide), F32),
        vm((tp, rows, width), BF16),
        vm((tp - 1, rows, width), BF16),
        pltpu.SemaphoreType.DMA((16 + kv,)),
        pltpu.SemaphoreType.DMA((4,)),
        pltpu.SemaphoreType.DMA((n_copies,)),
        pltpu.SemaphoreType.DMA((n_copies,)),
    ]
    anywhere = pl.BlockSpec(memory_space=pl.ANY)
    return pl.pallas_call(
        functools.partial(layer_kernel, kv, tp, subs),
        out_shape=(
            jax.ShapeDtypeStruct((rows, width), BF16),
            jax.ShapeDtypeStruct(cell_state.shape, F32),
            jax.ShapeDtypeStruct(norm_state.shape, F32),
            jax.ShapeDtypeStruct(max_state.shape, F32),
        ),
        in_specs=[anywhere] * len(operands),
        out_specs=(anywhere,) * 4,
        scratch_shapes=scratch,
        compiler_params=pltpu.CompilerParams(
            collective_id=0, has_side_effects=True, vmem_limit_bytes=60 * 1024 * 1024
        ),
    )(*operands)


def fits_kernel(kv, tp, *args):
    tokens, w_query, cell_state, w_up = args[0], args[2], args[10], args[15]
    return (
        kv > 1
        and tp > 1
        and tokens.shape[1] % 128 == 0
        and w_query.shape[0] % 256 == 0
        and w_query.shape[1] % 256 == 0
        and args[4].shape[1] % 256 == 0
        and cell_state.shape[0] % 8 == 0
        and 2 * cell_state.shape[0] <= 128
        and cell_state.shape[3] % 128 == 0
        and w_up.shape[1] % (512 * kv) == 0
        and args[6].shape[1] <= 128
    )


def on_device(kv, tp, *args):
    if fits_kernel(kv, tp, *args):
        return fused_on_device(kv, tp, *args)
    return plain_on_device(*args)


def solution(mesh):
    in_specs = (
        P("grp", ("kv", "tp")),
        P("kv"),
        P("kv", "tp"),
        P("kv", "tp"),
        P("kv", "tp"),
        P("kv", "tp"),
        P("kv", None),
        P("kv", None),
        P(),
        P(),
        P(("grp", "kv"), "tp", None, None),
        P(("grp", "kv"), "tp", None),
        P(("grp", "kv"), "tp"),
        P("tp", "kv"),
        P("kv"),
        P("kv", "tp"),
        P("tp", "kv"),
    )
    out_specs = (
        P("grp", ("kv", "tp")),
        P(("grp", "kv"), "tp", None, None),
        P(("grp", "kv"), "tp", None),
        P(("grp", "kv"), "tp"),
    )
    return jax.shard_map(
        functools.partial(on_device, mesh.shape["kv"], mesh.shape["tp"]),
        mesh=mesh, in_specs=in_specs, out_specs=out_specs, check_vma=False
    )
```

```python
import functools

import jax
import jax.numpy as jnp
from jax import lax
from jax.experimental import pallas as pl
from jax.experimental.pallas import tpu as pltpu
from jax.sharding import PartitionSpec as P

MESH = pl.DeviceIdType.MESH
BF16 = jnp.bfloat16
F32 = jnp.float32

EPSILON = 1e-06


def memory_step(
    query, keys, values, outgate, log_input, log_forget, cell_state, norm_state, max_state
):
    max_new = jnp.maximum(log_forget + max_state, log_input)
    keep = jnp.exp(log_forget + max_state - max_new)
    write = jnp.exp(log_input - max_new)
    cell_new = (
        keep[..., None, None] * cell_state
        + (write[..., None] * keys)[..., :, None] * values[..., None, :]
    )
    norm_new = keep[..., None] * norm_state + write[..., None] * keys
    numer = jnp.einsum("shk,shkv->shv", query, cell_new, precision=lax.Precision.HIGHEST)
    denom = jnp.maximum(jnp.abs(jnp.sum(query * norm_new, axis=-1)), jnp.exp(-max_new))
    heads = (jax.nn.sigmoid(outgate) * numer / denom[..., None]).astype(jnp.bfloat16)
    return (heads, cell_new, norm_new, max_new)


def matmul(left, right):
    return jnp.dot(left, right, preferred_element_type=jnp.float32)


def plain_on_device(
    tokens,
    gain_in,
    w_query,
    w_key,
    w_value,
    w_outgate,
    w_input_gate,
    w_forget_gate,
    bias_input,
    bias_forget,
    cell_state,
    norm_state,
    max_state,
    w_proj,
    gain_mid,
    w_up,
    w_down,
):
    seq_local, head_count = (cell_state.shape[0], cell_state.shape[1])
    key_dim, value_dim = (cell_state.shape[2], cell_state.shape[3])
    head_start = lax.axis_index("tp") * head_count
    column_width = tokens.shape[1]
    D = gain_in.shape[0] * lax.axis_size("kv")
    gathered = lax.all_gather(tokens, "tp", axis=1, tiled=True)
    widef = gathered.astype(jnp.float32)
    part_squares = jnp.sum(widef * widef, axis=1)
    normed = (widef * gain_in).astype(jnp.bfloat16)
    gate_input = lax.dynamic_slice_in_dim(w_input_gate, head_start, head_count, 1)
    gate_forget = lax.dynamic_slice_in_dim(w_forget_gate, head_start, head_count, 1)
    terms = jnp.concatenate(
        [
            matmul(normed, w_query),
            matmul(normed, w_key),
            matmul(normed, w_value),
            matmul(normed, w_outgate),
            matmul(normed, gate_input),
            matmul(normed, gate_forget),
        ],
        axis=1,
    )
    total_squares = lax.psum(part_squares, "kv")
    own_terms = lax.psum_scatter(terms, "kv", scatter_dimension=0, tiled=True)
    row_squares = lax.dynamic_slice_in_dim(
        total_squares, lax.axis_index("kv") * seq_local, seq_local, 0
    )
    own_terms = own_terms * lax.rsqrt(row_squares / D + EPSILON)[:, None]
    width_qk = head_count * key_dim
    width_v = head_count * value_dim
    query = own_terms[:, :width_qk].reshape(seq_local, head_count, key_dim) * key_dim ** (-0.5)
    keys = own_terms[:, width_qk : 2 * width_qk].reshape(seq_local, head_count, key_dim)
    offset = 2 * width_qk
    values = own_terms[:, offset : offset + width_v].reshape(seq_local, head_count, value_dim)
    offset = offset + width_v
    outgate = own_terms[:, offset : offset + width_v].reshape(seq_local, head_count, value_dim)
    offset = offset + width_v
    log_input = own_terms[:, offset : offset + head_count] + lax.dynamic_slice_in_dim(
        bias_input, head_start, head_count, 0
    )
    offset = offset + head_count
    log_forget = jax.nn.log_sigmoid(
        own_terms[:, offset : offset + head_count]
        + lax.dynamic_slice_in_dim(bias_forget, head_start, head_count, 0)
    )
    heads, cell_new, norm_new, max_new = memory_step(
        query, keys, values, outgate, log_input, log_forget, cell_state, norm_state, max_state
    )
    branch_part = matmul(
        lax.all_gather(heads.reshape(seq_local, width_v), "kv", axis=0, tiled=True), w_proj
    )
    branch = lax.psum(branch_part, "tp")
    middle = (widef + branch).astype(jnp.bfloat16)
    midf = middle.astype(jnp.float32)
    mid_squares = jnp.sum(midf * midf, axis=1)
    normed_mid = (midf * gain_mid).astype(jnp.bfloat16)
    up_part = matmul(normed_mid, w_up)
    up_rows, square_rows = (
        lax.psum_scatter(up_part, "kv", scatter_dimension=0, tiled=True),
        lax.psum_scatter(mid_squares, "kv", scatter_dimension=0, tiled=True),
    )
    upward = up_rows * lax.rsqrt(square_rows / D + EPSILON)[:, None]
    hidden = jnp.square(jax.nn.relu(upward)).astype(jnp.bfloat16)
    down_part = matmul(lax.all_gather(hidden, "kv", axis=0, tiled=True), w_down)
    own_down = lax.psum_scatter(
        down_part.astype(jnp.bfloat16), "tp", scatter_dimension=1, tiled=True
    ).astype(jnp.float32)
    residual = lax.dynamic_slice_in_dim(midf, lax.axis_index("tp") * column_width, column_width, 1)
    mixed = (residual + own_down).astype(jnp.bfloat16)
    return (mixed, cell_new, norm_new, max_new)


def matmul_nt(left, right):
    return lax.dot_general(left, right, (((1,), (1,)), ((), ())), preferred_element_type=F32)


class Exchange:
    def __init__(self, sems):
        self.send_sem, self.recv_sem = sems
        self.used = 0
        self.started = []

    def copy(self, axis, target, src, dst):
        index = self.used
        self.used += 1
        one = pltpu.make_async_remote_copy(
            src_ref=src,
            dst_ref=dst,
            send_sem=self.send_sem.at[index],
            recv_sem=self.recv_sem.at[index],
            device_id={axis: target},
            device_id_type=MESH,
        )
        one.start()
        self.started.append(one)
        return one


def partners(me, count):
    if count == 4:
        both = [3 - me, lax.rem(me + 2, 4), me + 1 - 2 * lax.rem(me, 2)]
        return both, both
    ahead = [lax.rem(me + o, count) for o in range(1, count)]
    behind = [lax.rem(me + count - o, count) for o in range(1, count)]
    return ahead, behind


def count_copies(kv, tp, subs):
    return 3 * (tp - 1) + 4 * (kv - 1) + 2 * subs * (kv - 1)


def layer_kernel(
    kv,
    tp,
    subs,
    tokens,
    gain_in,
    w_query,
    w_key,
    w_value,
    w_outgate,
    w_input_gate,
    w_forget_gate,
    bias_input,
    bias_forget,
    cell_state,
    norm_state,
    max_state,
    w_proj,
    gain_mid,
    w_up,
    w_down,
    mixed,
    cell_new,
    norm_new,
    max_new,
    tok,
    gain1,
    wqkv,
    wgi,
    wgf,
    bi,
    bf,
    cell,
    norm,
    mstate,
    wproj,
    gain2,
    wup,
    wdown,
    out_v,
    cell_o,
    norm_o,
    max_o,
    terms,
    b_send,
    b_recv,
    g_send,
    g_recv,
    numer,
    h_all,
    e_all,
    sq_all,
    mid,
    nmid,
    f_own,
    f_send,
    f_recv,
    hid,
    down,
    d_send,
    d_recv,
    in_sem,
    out_sem,
    send_sem,
    recv_sem,
):
    k_me, t_me = lax.axis_index("kv"), lax.axis_index("tp")
    link = Exchange((send_sem, recv_sem))
    rows, width = tok.shape[1], tok.shape[2]
    own_rows, n_heads, key_dim, value_dim = cell.shape
    wide = tp * width
    total_width = kv * wide
    w_qk, w_v = n_heads * key_dim, n_heads * value_dim
    half = f_own.shape[2]
    block = subs * half

    loads = []

    def load(src, dst):
        one = pltpu.make_async_copy(src, dst, in_sem.at[len(loads)])
        one.start()
        loads.append(one)
        return one

    l_tok = load(tokens, tok.at[t_me])
    l_gain = load(gain_in, gain1)
    l_q = load(w_query, wqkv.at[:, 0:w_qk])
    l_k = load(w_key, wqkv.at[:, w_qk : 2 * w_qk])
    l_v = load(w_value, wqkv.at[:, 2 * w_qk : 2 * w_qk + w_v])
    l_o = load(w_outgate, wqkv.at[:, 2 * w_qk + w_v : 2 * w_qk + 2 * w_v])
    l_gates = [load(w_input_gate, wgi), load(w_forget_gate, wgf)]
    l_small = [
        load(bias_input, bi),
        load(bias_forget, bf),
        load(norm_state, norm),
        load(max_state, mstate),
    ]
    l_cell = load(cell_state, cell)
    l_proj = load(w_proj, wproj)
    l_gain2 = load(gain_mid, gain2)
    l_up = load(w_up, wup)
    l_down = [
        load(w_down.at[pl.ds(i * block, block)], wdown.at[pl.ds(i * block, block)])
        for i in range(kv)
    ]

    barrier = pltpu.get_barrier_semaphore()
    k_peers, k_from = partners(k_me, kv)
    t_peers, t_from = partners(t_me, tp)
    for peer in t_peers:
        pl.semaphore_signal(barrier, inc=1, device_id={"tp": peer}, device_id_type=MESH)
    for peer in k_peers:
        pl.semaphore_signal(barrier, inc=1, device_id={"kv": peer}, device_id_type=MESH)
    g_send[...] = jnp.zeros_like(g_send)
    l_tok.wait()
    pl.semaphore_wait(barrier, kv + tp - 2)

    a_copies = [link.copy("tp", p, tok.at[t_me], tok.at[t_me]) for p in t_peers]
    l_gain.wait()
    for one in a_copies:
        one.wait_recv()
    wide_f = jnp.concatenate([tok[i] for i in range(tp)], axis=1).astype(F32)
    squares = jnp.sum(wide_f * wide_f, axis=1, keepdims=True)
    normed = (wide_f * gain1[...]).astype(BF16)

    for one in l_gates:
        one.wait()
    n_gates = wgi.shape[0]
    shape_g = (kv, own_rows, n_gates)
    g_send[:, :, 0:n_gates] = matmul_nt(normed, wgi[...]).reshape(shape_g)
    g_send[:, :, 128 : 128 + n_gates] = matmul_nt(normed, wgf[...]).reshape(shape_g)
    g_send[:, :, 256:384] = jnp.broadcast_to(squares, (rows, 128)).reshape(kv, own_rows, 128)
    g_copies = [
        link.copy("kv", p, g_send.at[p], g_recv.at[o]) for o, p in enumerate(k_peers)
    ]
    for one in (l_q, l_k, l_v, l_o):
        one.wait()
    tile = 256

    def project(i, carry):
        cols = pl.ds(pl.multiple_of(i * tile, tile), tile)
        part = matmul(normed, wqkv[:, cols]).reshape(kv, own_rows, tile)
        terms[:, :, cols] = part
        b_send[:, :, cols] = part.astype(BF16)
        return carry

    lax.fori_loop(0, wqkv.shape[1] // tile, project, 0)
    b_copies = [
        link.copy("kv", p, b_send.at[p], b_recv.at[o]) for o, p in enumerate(k_peers)
    ]

    for one in l_small:
        one.wait()
    l_cell.wait()
    for one in g_copies:
        one.wait_recv()
    gates = g_send[k_me]
    for o in range(kv - 1):
        gates = gates + g_recv[o]
    scale = lax.rsqrt(gates[:, 256:257] / total_width + EPSILON)
    log_i = gates[:, 0:n_gates] * scale + bi[...]
    raw_f = gates[:, 128 : 128 + n_gates] * scale + bf[...]
    log_f = jnp.minimum(raw_f, 0.0) - jnp.log1p(jnp.exp(-jnp.abs(raw_f)))
    gate_lane = lax.broadcasted_iota(jnp.int32, (own_rows, n_gates), 1)
    keep, write, floor = [], [], []
    max_cols = []
    old_max = mstate[...].T
    for h in range(n_heads):
        pick = gate_lane == t_me * n_heads + h
        li = jnp.sum(jnp.where(pick, log_i, 0.0), axis=1, keepdims=True)
        lf = jnp.sum(jnp.where(pick, log_f, 0.0), axis=1, keepdims=True)
        old = old_max[:, h : h + 1]
        new = jnp.maximum(lf + old, li)
        max_cols.append(new)
        keep.append(jnp.exp(lf + old - new))
        write.append(jnp.exp(li - new))
        floor.append(jnp.exp(-new))
    outs = []

    def store(src, dst):
        one = pltpu.make_async_copy(src, dst, out_sem.at[len(outs)])
        one.start()
        outs.append(one)

    head_lane = lax.broadcasted_iota(jnp.int32, (own_rows, n_heads), 1)
    new_max = jnp.broadcast_to(max_cols[0], (own_rows, n_heads))
    for h in range(1, n_heads):
        new_max = jnp.where(head_lane == h, max_cols[h], new_max)
    max_o[...] = new_max.T
    store(max_o, max_new)
    for one in b_copies:
        one.wait_recv()
    own = terms[k_me]
    for o in range(kv - 1):
        own = own + b_recv[o].astype(F32)
    own = own * scale
    query = own[:, 0:w_qk] * key_dim ** (-0.5)
    keys = own[:, w_qk : 2 * w_qk]
    values = own[:, 2 * w_qk : 2 * w_qk + w_v]
    outgate = own[:, 2 * w_qk + w_v : 2 * w_qk + 2 * w_v]
    qk_head = lax.broadcasted_iota(jnp.int32, (own_rows, w_qk), 1) // key_dim
    spread = jnp.broadcast_to(write[0], (own_rows, w_qk))
    for h in range(1, n_heads):
        spread = jnp.where(qk_head == h, write[h], spread)
    wkeys = keys * spread
    pad = jnp.zeros((128 - 2 * own_rows, w_qk), F32)
    turned = jnp.concatenate([wkeys, query, pad], axis=0).T
    denom, cross = [], []
    for h in range(n_heads):
        part = slice(h * key_dim, (h + 1) * key_dim)
        fresh = keep[h] * norm[:, h, :] + wkeys[:, part]
        norm_o[:, h, :] = fresh
        dot = jnp.sum(query[:, part] * fresh, axis=1, keepdims=True)
        shape_v = (own_rows, value_dim)
        denom.append(jnp.broadcast_to(jnp.maximum(jnp.abs(dot), floor[h]), shape_v))
        dot = jnp.sum(query[:, part] * wkeys[:, part], axis=1, keepdims=True)
        cross.append(jnp.broadcast_to(dot, shape_v))
    for h in range(n_heads):
        part = slice(h * key_dim, (h + 1) * key_dim)
        vals = slice(h * value_dim, (h + 1) * value_dim)
        for s in range(own_rows):
            q_col = turned[part, own_rows + s : own_rows + s + 1]
            numer[s : s + 1, vals] = jnp.sum(q_col * cell[s, h], axis=0, keepdims=True)
    keep_v = jnp.concatenate(
        [jnp.broadcast_to(one, (own_rows, value_dim)) for one in keep], axis=1
    )
    above = keep_v * numer[...] + jnp.concatenate(cross, axis=1) * values
    heads = jax.nn.sigmoid(outgate) * above / jnp.concatenate(denom, axis=1)
    h_all[k_me] = heads.astype(BF16)
    h_copies = [link.copy("kv", p, h_all.at[k_me], h_all.at[k_me]) for p in k_peers]
    store(norm_o, norm_new)
    for h in range(n_heads):
        part = slice(h * key_dim, (h + 1) * key_dim)
        vals = slice(h * value_dim, (h + 1) * value_dim)
        for s in range(own_rows):
            cell_o[s, h] = (
                keep[h][s : s + 1, :] * cell[s, h]
                + turned[part, s : s + 1] * values[s : s + 1, vals]
            )
    store(cell_o, cell_new)
    l_proj.wait()
    for one in h_copies:
        one.wait_recv()
    all_heads = jnp.concatenate([h_all[i].astype(F32) for i in range(kv)], axis=0)

    e_all[t_me] = matmul(all_heads.astype(BF16), wproj[...]).astype(BF16)
    e_copies = [link.copy("tp", p, e_all.at[t_me], e_all.at[t_me]) for p in t_peers]
    l_gain2.wait()
    for one in e_copies:
        one.wait_recv()
    branch = e_all[0].astype(F32)
    for i in range(1, tp):
        branch = branch + e_all[i].astype(F32)
    wide_f = jnp.concatenate([tok[i] for i in range(tp)], axis=1).astype(F32)
    middle = (wide_f + branch).astype(BF16).astype(F32)
    for i in range(tp):
        mid[i] = middle[:, i * width : (i + 1) * width]
    sq_all[k_me] = jnp.broadcast_to(jnp.sum(middle * middle, axis=1, keepdims=True), (rows, 128))
    s_copies = [link.copy("kv", p, sq_all.at[k_me], sq_all.at[k_me]) for p in k_peers]
    nmid[...] = (middle * gain2[...]).astype(BF16)

    l_up.wait()
    f_copies = {}

    def raise_block(target, sub, put):
        first = target * block + sub * half

        def raise_tile(i, carry):
            cols = pl.ds(pl.multiple_of(first + i * tile, tile), tile)
            put(pl.ds(pl.multiple_of(i * tile, tile), tile), matmul(nmid[...], wup[:, cols]))
            return carry

        lax.fori_loop(0, half // tile, raise_tile, 0)

    for sub in range(subs):
        for o, peer in enumerate(k_peers):

            def put_sent(here, part, o=o, sub=sub):
                f_send[o, sub, :, here] = part.astype(BF16)

            raise_block(peer, sub, put_sent)
            f_copies[o, sub] = link.copy("kv", peer, f_send.at[o, sub], f_recv.at[o, sub])
    for sub in range(subs):

        def put_own(here, part, sub=sub):
            f_own[sub, :, here] = part

        raise_block(k_me, sub, put_own)
    for one in s_copies:
        one.wait_recv()
    row_sum = sq_all[0, :, 0:1]
    for i in range(1, kv):
        row_sum = row_sum + sq_all[i, :, 0:1]
    scale_mid = lax.rsqrt(row_sum / total_width + EPSILON)
    g2_copies = {}
    for sub in range(subs):
        upward = f_own[sub]
        for o in range(kv - 1):
            f_copies[o, sub].wait_recv()
            upward = upward + f_recv[o, sub].astype(F32)
        hid[k_me, sub] = jnp.square(jnp.maximum(upward * scale_mid, 0.0)).astype(BF16)
        for o, peer in enumerate(k_peers):
            g2_copies[o, sub] = link.copy("kv", peer, hid.at[k_me, sub], hid.at[k_me, sub])

    for one in l_down:
        one.wait()

    def lower_block(source, sub, first):
        deep = pl.ds(pl.multiple_of(source * block + sub * half, half), half)
        part = matmul(hid[source, sub], wdown[deep, :])
        down[...] = part if first else down[...] + part

    for sub in range(subs):
        lower_block(k_me, sub, sub == 0)
    for sub in range(subs):
        for o in list(range(kv - 1))[::-1]:
            g2_copies[o, sub].wait_recv()
            lower_block(k_from[o], sub, False)
    for i in range(tp):
        d_send[i] = down[:, i * width : (i + 1) * width].astype(BF16)
    d_copies = [
        link.copy("tp", p, d_send.at[p], d_recv.at[o]) for o, p in enumerate(t_peers)
    ]
    lower = d_send[t_me].astype(F32)
    for o, one in enumerate(d_copies):
        one.wait_recv()
        lower = lower + d_recv[o].astype(F32)
    out_v[...] = (mid[t_me] + lower).astype(BF16)
    store(out_v, mixed)
    for one in link.started:
        one.wait_send()
    for one in outs:
        one.wait()


def finish_kernel(*refs):
    sources, outs, stage = refs[0:4], refs[4:8], refs[8:12]
    in_sem, out_sem = refs[12:]
    pieces = [(sources[i], stage[i], outs[i]) for i in (0, 2, 3)]
    for s in range(sources[1].shape[0]):
        pieces.append((sources[1].at[s], stage[1].at[s], outs[1].at[s]))
    inward = [pltpu.make_async_copy(p[0], p[1], in_sem.at[i]) for i, p in enumerate(pieces)]
    outward = [pltpu.make_async_copy(p[1], p[2], out_sem.at[i]) for i, p in enumerate(pieces)]
    for one in inward:
        one.start()
    for one, two in zip(inward, outward):
        one.wait()
        two.start()
    for two in outward:
        two.wait()


def fused_on_device(kv, tp, *args):
    (tokens, gain_in, w_query, w_key, w_value, w_outgate, w_input_gate, w_forget_gate) = args[:8]
    (bias_input, bias_forget, cell_state, norm_state, max_state) = args[8:13]
    (w_proj, gain_mid, w_up, w_down) = args[13:]
    rows, width = tokens.shape
    own_rows = cell_state.shape[0]
    wide = w_query.shape[0]
    n_qkv = w_query.shape[1] + w_key.shape[1] + w_value.shape[1] + w_outgate.shape[1]
    hidden = w_up.shape[1]
    subs = 4 if hidden % (1024 * kv) == 0 else 2
    half = hidden // (kv * subs)
    w_v = w_value.shape[1]
    operands = (
        tokens,
        gain_in.reshape(1, -1),
        w_query,
        w_key,
        w_value,
        w_outgate,
        w_input_gate.T,
        w_forget_gate.T,
        bias_input.reshape(1, -1),
        bias_forget.reshape(1, -1),
        cell_state,
        norm_state,
        max_state.T,
        w_proj,
        gain_mid.reshape(1, -1),
        w_up,
        w_down,
    )
    n_copies = count_copies(kv, tp, subs)
    vm = pltpu.VMEM
    scratch = [
        vm((tp, rows, width), BF16),
        vm((1, wide), F32),
        vm((wide, n_qkv), BF16),
        vm(w_input_gate.shape[::-1], BF16),
        vm(w_forget_gate.shape[::-1], BF16),
        vm((1, bias_input.shape[0]), F32),
        vm((1, bias_forget.shape[0]), F32),
        vm(cell_state.shape, F32),
        vm(norm_state.shape, F32),
        vm(max_state.shape[::-1], F32),
        vm(w_proj.shape, BF16),
        vm((1, wide), F32),
        vm(w_up.shape, BF16),
        vm(w_down.shape, BF16),
        vm((rows, width), BF16),
        vm(cell_state.shape, F32),
        vm(norm_state.shape, F32),
        vm(max_state.shape[::-1], F32),
        vm((kv, own_rows, n_qkv), F32),
        vm((kv, own_rows, n_qkv), BF16),
        vm((kv - 1, own_rows, n_qkv), BF16),
        vm((kv, own_rows, 384), F32),
        vm((kv - 1, own_rows, 384), F32),
        vm((own_rows, w_v), F32),
        vm((kv, own_rows, w_v), BF16),
        vm((tp, rows, wide), BF16),
        vm((kv, rows, 128), F32),
        vm((tp, rows, width), F32),
        vm((rows, wide), BF16),
        vm((subs, rows, half), F32),
        vm((kv - 1, subs, rows, half), BF16),
        vm((kv - 1, subs, rows, half), BF16),
        vm((kv, subs, rows, half), BF16),
        vm((rows, wide), F32),
        vm((tp, rows, width), BF16),
        vm((tp - 1, rows, width), BF16),
        pltpu.SemaphoreType.DMA((16 + kv,)),
        pltpu.SemaphoreType.DMA((4,)),
        pltpu.SemaphoreType.DMA((n_copies,)),
        pltpu.SemaphoreType.DMA((n_copies,)),
    ]
    anywhere = pl.BlockSpec(memory_space=pl.ANY)
    results = pl.pallas_call(
        functools.partial(layer_kernel, kv, tp, subs),
        out_shape=(
            jax.ShapeDtypeStruct((rows, width), BF16),
            jax.ShapeDtypeStruct(cell_state.shape, F32),
            jax.ShapeDtypeStruct(norm_state.shape, F32),
            jax.ShapeDtypeStruct(max_state.shape[::-1], F32),
        ),
        in_specs=[anywhere] * len(operands),
        out_specs=(anywhere,) * 4,
        scratch_shapes=scratch,
        compiler_params=pltpu.CompilerParams(
            collective_id=0, has_side_effects=True, vmem_limit_bytes=60 * 1024 * 1024
        ),
    )(*operands)
    mixed, cell_new, norm_new, max_new = pl.pallas_call(
        finish_kernel,
        out_shape=tuple(jax.ShapeDtypeStruct(one.shape, one.dtype) for one in results),
        in_specs=[anywhere] * 4,
        out_specs=(anywhere,) * 4,
        scratch_shapes=[vm(one.shape, one.dtype) for one in results]
        + [pltpu.SemaphoreType.DMA((3 + own_rows,))] * 2,
        compiler_params=pltpu.CompilerParams(vmem_limit_bytes=60 * 1024 * 1024),
    )(*results)
    return (mixed, cell_new, norm_new, max_new.T)


def fits_kernel(kv, tp, *args):
    tokens, w_query, cell_state, w_up = args[0], args[2], args[10], args[15]
    return (
        kv > 1
        and tp > 1
        and tokens.shape[1] % 128 == 0
        and w_query.shape[0] % 256 == 0
        and w_query.shape[1] % 256 == 0
        and args[4].shape[1] % 256 == 0
        and cell_state.shape[0] % 8 == 0
        and 2 * cell_state.shape[0] <= 128
        and cell_state.shape[3] % 128 == 0
        and w_up.shape[1] % (512 * kv) == 0
        and args[6].shape[1] <= 128
    )


def on_device(kv, tp, *args):
    if fits_kernel(kv, tp, *args):
        return fused_on_device(kv, tp, *args)
    return plain_on_device(*args)


def solution(mesh):
    in_specs = (
        P("grp", ("kv", "tp")),
        P("kv"),
        P("kv", "tp"),
        P("kv", "tp"),
        P("kv", "tp"),
        P("kv", "tp"),
        P("kv", None),
        P("kv", None),
        P(),
        P(),
        P(("grp", "kv"), "tp", None, None),
        P(("grp", "kv"), "tp", None),
        P(("grp", "kv"), "tp"),
        P("tp", "kv"),
        P("kv"),
        P("kv", "tp"),
        P("tp", "kv"),
    )
    out_specs = (
        P("grp", ("kv", "tp")),
        P(("grp", "kv"), "tp", None, None),
        P(("grp", "kv"), "tp", None),
        P(("grp", "kv"), "tp"),
    )
    return jax.shard_map(
        functools.partial(on_device, mesh.shape["kv"], mesh.shape["tp"]),
        mesh=mesh, in_specs=in_specs, out_specs=out_specs, check_vma=False
    )
```

```python
import functools

import jax
import jax.numpy as jnp
from jax import lax
from jax.experimental import pallas as pl
from jax.experimental.pallas import tpu as pltpu
from jax.sharding import PartitionSpec as P

MESH = pl.DeviceIdType.MESH
BF16 = jnp.bfloat16
F32 = jnp.float32

EPSILON = 1e-06


def memory_step(
    query, keys, values, outgate, log_input, log_forget, cell_state, norm_state, max_state
):
    max_new = jnp.maximum(log_forget + max_state, log_input)
    keep = jnp.exp(log_forget + max_state - max_new)
    write = jnp.exp(log_input - max_new)
    cell_new = (
        keep[..., None, None] * cell_state
        + (write[..., None] * keys)[..., :, None] * values[..., None, :]
    )
    norm_new = keep[..., None] * norm_state + write[..., None] * keys
    numer = jnp.einsum("shk,shkv->shv", query, cell_new, precision=lax.Precision.HIGHEST)
    denom = jnp.maximum(jnp.abs(jnp.sum(query * norm_new, axis=-1)), jnp.exp(-max_new))
    heads = (jax.nn.sigmoid(outgate) * numer / denom[..., None]).astype(jnp.bfloat16)
    return (heads, cell_new, norm_new, max_new)


def matmul(left, right):
    return jnp.dot(left, right, preferred_element_type=jnp.float32)


def plain_on_device(
    tokens,
    gain_in,
    w_query,
    w_key,
    w_value,
    w_outgate,
    w_input_gate,
    w_forget_gate,
    bias_input,
    bias_forget,
    cell_state,
    norm_state,
    max_state,
    w_proj,
    gain_mid,
    w_up,
    w_down,
):
    seq_local, head_count = (cell_state.shape[0], cell_state.shape[1])
    key_dim, value_dim = (cell_state.shape[2], cell_state.shape[3])
    head_start = lax.axis_index("tp") * head_count
    column_width = tokens.shape[1]
    D = gain_in.shape[0] * lax.axis_size("kv")
    gathered = lax.all_gather(tokens, "tp", axis=1, tiled=True)
    widef = gathered.astype(jnp.float32)
    part_squares = jnp.sum(widef * widef, axis=1)
    normed = (widef * gain_in).astype(jnp.bfloat16)
    gate_input = lax.dynamic_slice_in_dim(w_input_gate, head_start, head_count, 1)
    gate_forget = lax.dynamic_slice_in_dim(w_forget_gate, head_start, head_count, 1)
    terms = jnp.concatenate(
        [
            matmul(normed, w_query),
            matmul(normed, w_key),
            matmul(normed, w_value),
            matmul(normed, w_outgate),
            matmul(normed, gate_input),
            matmul(normed, gate_forget),
        ],
        axis=1,
    )
    total_squares = lax.psum(part_squares, "kv")
    own_terms = lax.psum_scatter(terms, "kv", scatter_dimension=0, tiled=True)
    row_squares = lax.dynamic_slice_in_dim(
        total_squares, lax.axis_index("kv") * seq_local, seq_local, 0
    )
    own_terms = own_terms * lax.rsqrt(row_squares / D + EPSILON)[:, None]
    width_qk = head_count * key_dim
    width_v = head_count * value_dim
    query = own_terms[:, :width_qk].reshape(seq_local, head_count, key_dim) * key_dim ** (-0.5)
    keys = own_terms[:, width_qk : 2 * width_qk].reshape(seq_local, head_count, key_dim)
    offset = 2 * width_qk
    values = own_terms[:, offset : offset + width_v].reshape(seq_local, head_count, value_dim)
    offset = offset + width_v
    outgate = own_terms[:, offset : offset + width_v].reshape(seq_local, head_count, value_dim)
    offset = offset + width_v
    log_input = own_terms[:, offset : offset + head_count] + lax.dynamic_slice_in_dim(
        bias_input, head_start, head_count, 0
    )
    offset = offset + head_count
    log_forget = jax.nn.log_sigmoid(
        own_terms[:, offset : offset + head_count]
        + lax.dynamic_slice_in_dim(bias_forget, head_start, head_count, 0)
    )
    heads, cell_new, norm_new, max_new = memory_step(
        query, keys, values, outgate, log_input, log_forget, cell_state, norm_state, max_state
    )
    branch_part = matmul(
        lax.all_gather(heads.reshape(seq_local, width_v), "kv", axis=0, tiled=True), w_proj
    )
    branch = lax.psum(branch_part, "tp")
    middle = (widef + branch).astype(jnp.bfloat16)
    midf = middle.astype(jnp.float32)
    mid_squares = jnp.sum(midf * midf, axis=1)
    normed_mid = (midf * gain_mid).astype(jnp.bfloat16)
    up_part = matmul(normed_mid, w_up)
    up_rows, square_rows = (
        lax.psum_scatter(up_part, "kv", scatter_dimension=0, tiled=True),
        lax.psum_scatter(mid_squares, "kv", scatter_dimension=0, tiled=True),
    )
    upward = up_rows * lax.rsqrt(square_rows / D + EPSILON)[:, None]
    hidden = jnp.square(jax.nn.relu(upward)).astype(jnp.bfloat16)
    down_part = matmul(lax.all_gather(hidden, "kv", axis=0, tiled=True), w_down)
    own_down = lax.psum_scatter(
        down_part.astype(jnp.bfloat16), "tp", scatter_dimension=1, tiled=True
    ).astype(jnp.float32)
    residual = lax.dynamic_slice_in_dim(midf, lax.axis_index("tp") * column_width, column_width, 1)
    mixed = (residual + own_down).astype(jnp.bfloat16)
    return (mixed, cell_new, norm_new, max_new)


def matmul_nt(left, right):
    return lax.dot_general(left, right, (((1,), (1,)), ((), ())), preferred_element_type=F32)


class Exchange:
    def __init__(self, sems):
        self.send_sem, self.recv_sem = sems
        self.used = 0
        self.started = []

    def copy(self, axis, target, src, dst, when=None):
        index = self.used
        self.used += 1
        one = pltpu.make_async_remote_copy(
            src_ref=src,
            dst_ref=dst,
            send_sem=self.send_sem.at[index],
            recv_sem=self.recv_sem.at[index],
            device_id={axis: target},
            device_id_type=MESH,
        )
        if when is None:
            one.start()
        else:
            pl.when(when)(one.start)
        self.started.append(one)
        return one


def partners(me, count):
    if count == 4:
        both = [3 - me, lax.rem(me + 2, 4), me + 1 - 2 * lax.rem(me, 2)]
        return both, both
    ahead = [lax.rem(me + o, count) for o in range(1, count)]
    behind = [lax.rem(me + count - o, count) for o in range(1, count)]
    return ahead, behind


def count_copies(kv, tp, subs):
    return 3 * (tp - 1) + 4 * (kv - 1) + 2 * subs * (kv - 1)


def layer_kernel(
    kv,
    tp,
    subs,
    tokens,
    gain_in,
    w_query,
    w_key,
    w_value,
    w_outgate,
    w_input_gate,
    w_forget_gate,
    bias_input,
    bias_forget,
    cell_state,
    norm_state,
    max_state,
    w_proj,
    gain_mid,
    w_up,
    w_down,
    mixed,
    cell_new,
    norm_new,
    max_new,
    tok,
    gain1,
    wqkv,
    wgi,
    wgf,
    bi,
    bf,
    cell,
    norm,
    mstate,
    wproj,
    gain2,
    wup,
    wdown,
    out_v,
    cell_o,
    norm_o,
    max_o,
    terms,
    b_send,
    b_recv,
    g_send,
    g_recv,
    numer,
    h_all,
    e_all,
    sq_all,
    mid,
    nmid,
    f_own,
    f_send,
    f_recv,
    hid,
    down,
    d_send,
    d_recv,
    in_sem,
    out_sem,
    send_sem,
    recv_sem,
):
    k_me, t_me = lax.axis_index("kv"), lax.axis_index("tp")
    link = Exchange((send_sem, recv_sem))
    rows, width = tok.shape[1], tok.shape[2]
    own_rows, n_heads, key_dim, value_dim = cell.shape
    wide = tp * width
    total_width = kv * wide
    w_qk, w_v = n_heads * key_dim, n_heads * value_dim
    half = f_own.shape[2]
    block = subs * half

    loads = []

    def load(src, dst):
        one = pltpu.make_async_copy(src, dst, in_sem.at[len(loads)])
        one.start()
        loads.append(one)
        return one

    l_tok = load(tokens, tok.at[t_me])
    l_gain = load(gain_in, gain1)
    l_q = load(w_query, wqkv.at[:, 0:w_qk])
    l_k = load(w_key, wqkv.at[:, w_qk : 2 * w_qk])
    l_v = load(w_value, wqkv.at[:, 2 * w_qk : 2 * w_qk + w_v])
    l_o = load(w_outgate, wqkv.at[:, 2 * w_qk + w_v : 2 * w_qk + 2 * w_v])
    l_gates = [load(w_input_gate, wgi), load(w_forget_gate, wgf)]
    l_small = [
        load(bias_input, bi),
        load(bias_forget, bf),
        load(norm_state, norm),
        load(max_state, mstate),
    ]

    barrier = pltpu.get_barrier_semaphore()
    k_peers, k_from = partners(k_me, kv)
    t_peers, t_from = partners(t_me, tp)
    for peer in t_peers:
        pl.semaphore_signal(barrier, inc=1, device_id={"tp": peer}, device_id_type=MESH)
    for peer in k_peers:
        pl.semaphore_signal(barrier, inc=1, device_id={"kv": peer}, device_id_type=MESH)
    g_send[...] = jnp.zeros_like(g_send)
    l_tok.wait()
    pl.semaphore_wait(barrier, kv + tp - 2)

    a_copies = [link.copy("tp", p, tok.at[t_me], tok.at[t_me]) for p in t_peers]
    l_cell = load(cell_state, cell)
    l_proj = load(w_proj, wproj)
    l_gain2 = load(gain_mid, gain2)
    l_up = load(w_up, wup)
    l_down = [
        load(w_down.at[pl.ds(i * block, block)], wdown.at[pl.ds(i * block, block)])
        for i in range(kv)
    ]
    l_gain.wait()
    for one in a_copies:
        one.wait_recv()
    wide_f = jnp.concatenate([tok[i] for i in range(tp)], axis=1).astype(F32)
    squares = jnp.sum(wide_f * wide_f, axis=1, keepdims=True)
    normed = (wide_f * gain1[...]).astype(BF16)

    for one in l_gates:
        one.wait()
    n_gates = wgi.shape[0]
    shape_g = (kv, own_rows, n_gates)
    g_send[:, :, 0:n_gates] = matmul_nt(normed, wgi[...]).reshape(shape_g)
    g_send[:, :, 128 : 128 + n_gates] = matmul_nt(normed, wgf[...]).reshape(shape_g)
    g_send[:, :, 256:384] = jnp.broadcast_to(squares, (rows, 128)).reshape(kv, own_rows, 128)
    g_copies = [
        link.copy("kv", p, g_send.at[p], g_recv.at[o]) for o, p in enumerate(k_peers)
    ]
    for one in (l_q, l_k, l_v, l_o):
        one.wait()
    tile = 256

    def project(i, carry):
        cols = pl.ds(pl.multiple_of(i * tile, tile), tile)
        part = matmul(normed, wqkv[:, cols]).reshape(kv, own_rows, tile)
        terms[:, :, cols] = part
        b_send[:, :, cols] = part.astype(BF16)
        return carry

    lax.fori_loop(0, wqkv.shape[1] // tile, project, 0)
    b_copies = [
        link.copy("kv", p, b_send.at[p], b_recv.at[o]) for o, p in enumerate(k_peers)
    ]

    for one in l_small:
        one.wait()
    l_cell.wait()
    for one in g_copies:
        one.wait_recv()
    gates = g_send[k_me]
    for o in range(kv - 1):
        gates = gates + g_recv[o]
    scale = lax.rsqrt(gates[:, 256:257] / total_width + EPSILON)
    log_i = gates[:, 0:n_gates] * scale + bi[...]
    raw_f = gates[:, 128 : 128 + n_gates] * scale + bf[...]
    log_f = jnp.minimum(raw_f, 0.0) - jnp.log1p(jnp.exp(-jnp.abs(raw_f)))
    gate_lane = lax.broadcasted_iota(jnp.int32, (own_rows, n_gates), 1)
    keep, write, floor = [], [], []
    max_cols = []
    old_max = mstate[...].T
    for h in range(n_heads):
        pick = gate_lane == t_me * n_heads + h
        li = jnp.sum(jnp.where(pick, log_i, 0.0), axis=1, keepdims=True)
        lf = jnp.sum(jnp.where(pick, log_f, 0.0), axis=1, keepdims=True)
        old = old_max[:, h : h + 1]
        new = jnp.maximum(lf + old, li)
        max_cols.append(new)
        keep.append(jnp.exp(lf + old - new))
        write.append(jnp.exp(li - new))
        floor.append(jnp.exp(-new))
    outs = []

    def store(src, dst):
        one = pltpu.make_async_copy(src, dst, out_sem.at[len(outs)])
        one.start()
        outs.append(one)

    head_lane = lax.broadcasted_iota(jnp.int32, (own_rows, n_heads), 1)
    new_max = jnp.broadcast_to(max_cols[0], (own_rows, n_heads))
    for h in range(1, n_heads):
        new_max = jnp.where(head_lane == h, max_cols[h], new_max)
    max_o[...] = new_max.T
    store(max_o, max_new)
    for one in b_copies:
        one.wait_recv()
    own = terms[k_me]
    for o in range(kv - 1):
        own = own + b_recv[o].astype(F32)
    own = own * scale
    query = own[:, 0:w_qk] * key_dim ** (-0.5)
    keys = own[:, w_qk : 2 * w_qk]
    values = own[:, 2 * w_qk : 2 * w_qk + w_v]
    outgate = own[:, 2 * w_qk + w_v : 2 * w_qk + 2 * w_v]
    qk_head = lax.broadcasted_iota(jnp.int32, (own_rows, w_qk), 1) // key_dim
    spread = jnp.broadcast_to(write[0], (own_rows, w_qk))
    for h in range(1, n_heads):
        spread = jnp.where(qk_head == h, write[h], spread)
    wkeys = keys * spread
    pad = jnp.zeros((128 - 2 * own_rows, w_qk), F32)
    turned = jnp.concatenate([wkeys, query, pad], axis=0).T
    denom, cross = [], []
    for h in range(n_heads):
        part = slice(h * key_dim, (h + 1) * key_dim)
        fresh = keep[h] * norm[:, h, :] + wkeys[:, part]
        norm_o[:, h, :] = fresh
        dot = jnp.sum(query[:, part] * fresh, axis=1, keepdims=True)
        shape_v = (own_rows, value_dim)
        denom.append(jnp.broadcast_to(jnp.maximum(jnp.abs(dot), floor[h]), shape_v))
        dot = jnp.sum(query[:, part] * wkeys[:, part], axis=1, keepdims=True)
        cross.append(jnp.broadcast_to(dot, shape_v))
    for h in range(n_heads):
        part = slice(h * key_dim, (h + 1) * key_dim)
        vals = slice(h * value_dim, (h + 1) * value_dim)
        for s in range(own_rows):
            q_col = turned[part, own_rows + s : own_rows + s + 1]
            numer[s : s + 1, vals] = jnp.sum(q_col * cell[s, h], axis=0, keepdims=True)
    keep_v = jnp.concatenate(
        [jnp.broadcast_to(one, (own_rows, value_dim)) for one in keep], axis=1
    )
    above = keep_v * numer[...] + jnp.concatenate(cross, axis=1) * values
    heads = jax.nn.sigmoid(outgate) * above / jnp.concatenate(denom, axis=1)
    h_all[k_me] = heads.astype(BF16)
    h_copies = [link.copy("kv", p, h_all.at[k_me], h_all.at[k_me]) for p in k_peers]
    store(norm_o, norm_new)
    for h in range(n_heads):
        part = slice(h * key_dim, (h + 1) * key_dim)
        vals = slice(h * value_dim, (h + 1) * value_dim)
        for s in range(own_rows):
            cell_o[s, h] = (
                keep[h][s : s + 1, :] * cell[s, h]
                + turned[part, s : s + 1] * values[s : s + 1, vals]
            )
    store(cell_o, cell_new)
    l_proj.wait()
    for one in h_copies:
        one.wait_recv()
    all_heads = jnp.concatenate([h_all[i].astype(F32) for i in range(kv)], axis=0)

    e_all[t_me] = matmul(all_heads.astype(BF16), wproj[...]).astype(BF16)
    e_copies = [link.copy("tp", p, e_all.at[t_me], e_all.at[t_me]) for p in t_peers]
    l_gain2.wait()
    for one in e_copies:
        one.wait_recv()
    branch = e_all[0].astype(F32)
    for i in range(1, tp):
        branch = branch + e_all[i].astype(F32)
    wide_f = jnp.concatenate([tok[i] for i in range(tp)], axis=1).astype(F32)
    middle = (wide_f + branch).astype(BF16).astype(F32)
    for i in range(tp):
        mid[i] = middle[:, i * width : (i + 1) * width]
    sq_all[k_me] = jnp.broadcast_to(jnp.sum(middle * middle, axis=1, keepdims=True), (rows, 128))
    s_copies = [link.copy("kv", p, sq_all.at[k_me], sq_all.at[k_me]) for p in k_peers]
    nmid[...] = (middle * gain2[...]).astype(BF16)

    l_up.wait()
    f_copies = {}

    def raise_block(target, sub, put):
        first = target * block + sub * half

        def raise_tile(i, carry):
            cols = pl.ds(pl.multiple_of(first + i * tile, tile), tile)
            put(pl.ds(pl.multiple_of(i * tile, tile), tile), matmul(nmid[...], wup[:, cols]))
            return carry

        lax.fori_loop(0, half // tile, raise_tile, 0)

    is_end = jnp.logical_or(k_me == 0, k_me == kv - 1)
    is_mid = jnp.logical_not(is_end)
    across, skip, near = k_peers
    targets = [across, jnp.where(is_end, near, skip), near]
    for o in (1, 0, 2):
        for sub in range(subs):

            def put_sent(here, part, o=o, sub=sub):
                f_send[o, sub, :, here] = part.astype(BF16)

            raise_block(k_peers[o], sub, put_sent)
            f_copies[o, sub] = link.copy(
                "kv",
                targets[o],
                f_send.at[o, sub],
                f_recv.at[o, sub],
                when=None if o else is_end,
            )
    for sub in range(subs):
        f_copies[1, sub].wait_recv()

        def relay(sub=sub):
            both = f_send[0, sub].astype(F32) + f_recv[1, sub].astype(F32)
            f_send[0, sub] = both.astype(BF16)
            f_copies[0, sub].start()

        pl.when(is_mid)(relay)

        def put_own(here, part, sub=sub):
            f_own[sub, :, here] = part

        raise_block(k_me, sub, put_own)
    for one in s_copies:
        one.wait_recv()
    row_sum = sq_all[0, :, 0:1]
    for i in range(1, kv):
        row_sum = row_sum + sq_all[i, :, 0:1]
    scale_mid = lax.rsqrt(row_sum / total_width + EPSILON)
    g2_copies = {}
    for sub in range(subs):
        upward = f_own[sub]
        f_copies[0, sub].wait_recv()
        f_copies[2, sub].wait_recv()
        skipped = jnp.where(is_end, f_recv[1, sub].astype(F32), 0.0)
        upward = upward + f_recv[0, sub].astype(F32) + skipped + f_recv[2, sub].astype(F32)
        hid[k_me, sub] = jnp.square(jnp.maximum(upward * scale_mid, 0.0)).astype(BF16)
        mine = hid.at[k_me, sub]
        g2_copies[0, sub] = link.copy("kv", across, mine, mine)
        carried = hid.at[jnp.where(is_end, k_me, across), sub]
        to = jnp.where(is_end, skip, near)
        g2_copies[1, sub] = link.copy("kv", to, carried, carried, when=is_end)
        g2_copies[2, sub] = link.copy("kv", near, mine, mine)

    for one in l_down:
        one.wait()

    def lower_block(source, sub, first):
        deep = pl.ds(pl.multiple_of(source * block + sub * half, half), half)
        part = matmul(hid[source, sub], wdown[deep, :])
        down[...] = part if first else down[...] + part

    for sub in range(subs):
        lower_block(k_me, sub, sub == 0)
    for sub in range(subs):
        g2_copies[0, sub].wait_recv()
        pl.when(is_mid)(g2_copies[1, sub].start)
        lower_block(across, sub, False)
        g2_copies[2, sub].wait_recv()
        lower_block(near, sub, False)
    for sub in range(subs):
        g2_copies[1, sub].wait_recv()
        lower_block(skip, sub, False)
    for i in range(tp):
        d_send[i] = down[:, i * width : (i + 1) * width].astype(BF16)
    d_copies = [
        link.copy("tp", p, d_send.at[p], d_recv.at[o]) for o, p in enumerate(t_peers)
    ]
    lower = d_send[t_me].astype(F32)
    for o, one in enumerate(d_copies):
        one.wait_recv()
        lower = lower + d_recv[o].astype(F32)
    out_v[...] = (mid[t_me] + lower).astype(BF16)
    store(out_v, mixed)
    for one in link.started:
        one.wait_send()
    for one in outs:
        one.wait()


def finish_kernel(*refs):
    sources, outs, stage = refs[0:4], refs[4:8], refs[8:12]
    in_sem, out_sem = refs[12:]
    pieces = [(sources[i], stage[i], outs[i]) for i in (0, 2, 3)]
    for s in range(sources[1].shape[0]):
        pieces.append((sources[1].at[s], stage[1].at[s], outs[1].at[s]))
    inward = [pltpu.make_async_copy(p[0], p[1], in_sem.at[i]) for i, p in enumerate(pieces)]
    outward = [pltpu.make_async_copy(p[1], p[2], out_sem.at[i]) for i, p in enumerate(pieces)]
    for one in inward:
        one.start()
    for one, two in zip(inward, outward):
        one.wait()
        two.start()
    for two in outward:
        two.wait()


def fused_on_device(kv, tp, *args):
    (tokens, gain_in, w_query, w_key, w_value, w_outgate, w_input_gate, w_forget_gate) = args[:8]
    (bias_input, bias_forget, cell_state, norm_state, max_state) = args[8:13]
    (w_proj, gain_mid, w_up, w_down) = args[13:]
    rows, width = tokens.shape
    own_rows = cell_state.shape[0]
    wide = w_query.shape[0]
    n_qkv = w_query.shape[1] + w_key.shape[1] + w_value.shape[1] + w_outgate.shape[1]
    hidden = w_up.shape[1]
    subs = 4 if hidden % (1024 * kv) == 0 else 2
    half = hidden // (kv * subs)
    w_v = w_value.shape[1]
    operands = (
        tokens,
        gain_in.reshape(1, -1),
        w_query,
        w_key,
        w_value,
        w_outgate,
        w_input_gate.T,
        w_forget_gate.T,
        bias_input.reshape(1, -1),
        bias_forget.reshape(1, -1),
        cell_state,
        norm_state,
        max_state.T,
        w_proj,
        gain_mid.reshape(1, -1),
        w_up,
        w_down,
    )
    n_copies = count_copies(kv, tp, subs)
    vm = pltpu.VMEM
    scratch = [
        vm((tp, rows, width), BF16),
        vm((1, wide), F32),
        vm((wide, n_qkv), BF16),
        vm(w_input_gate.shape[::-1], BF16),
        vm(w_forget_gate.shape[::-1], BF16),
        vm((1, bias_input.shape[0]), F32),
        vm((1, bias_forget.shape[0]), F32),
        vm(cell_state.shape, F32),
        vm(norm_state.shape, F32),
        vm(max_state.shape[::-1], F32),
        vm(w_proj.shape, BF16),
        vm((1, wide), F32),
        vm(w_up.shape, BF16),
        vm(w_down.shape, BF16),
        vm((rows, width), BF16),
        vm(cell_state.shape, F32),
        vm(norm_state.shape, F32),
        vm(max_state.shape[::-1], F32),
        vm((kv, own_rows, n_qkv), F32),
        vm((kv, own_rows, n_qkv), BF16),
        vm((kv - 1, own_rows, n_qkv), BF16),
        vm((kv, own_rows, 384), F32),
        vm((kv - 1, own_rows, 384), F32),
        vm((own_rows, w_v), F32),
        vm((kv, own_rows, w_v), BF16),
        vm((tp, rows, wide), BF16),
        vm((kv, rows, 128), F32),
        vm((tp, rows, width), F32),
        vm((rows, wide), BF16),
        vm((subs, rows, half), F32),
        vm((kv - 1, subs, rows, half), BF16),
        vm((kv - 1, subs, rows, half), BF16),
        vm((kv, subs, rows, half), BF16),
        vm((rows, wide), F32),
        vm((tp, rows, width), BF16),
        vm((tp - 1, rows, width), BF16),
        pltpu.SemaphoreType.DMA((16 + kv,)),
        pltpu.SemaphoreType.DMA((4,)),
        pltpu.SemaphoreType.DMA((n_copies,)),
        pltpu.SemaphoreType.DMA((n_copies,)),
    ]
    anywhere = pl.BlockSpec(memory_space=pl.ANY)
    results = pl.pallas_call(
        functools.partial(layer_kernel, kv, tp, subs),
        out_shape=(
            jax.ShapeDtypeStruct((rows, width), BF16),
            jax.ShapeDtypeStruct(cell_state.shape, F32),
            jax.ShapeDtypeStruct(norm_state.shape, F32),
            jax.ShapeDtypeStruct(max_state.shape[::-1], F32),
        ),
        in_specs=[anywhere] * len(operands),
        out_specs=(anywhere,) * 4,
        scratch_shapes=scratch,
        compiler_params=pltpu.CompilerParams(
            collective_id=0, has_side_effects=True, vmem_limit_bytes=60 * 1024 * 1024
        ),
    )(*operands)
    mixed, cell_new, norm_new, max_new = pl.pallas_call(
        finish_kernel,
        out_shape=tuple(jax.ShapeDtypeStruct(one.shape, one.dtype) for one in results),
        in_specs=[anywhere] * 4,
        out_specs=(anywhere,) * 4,
        scratch_shapes=[vm(one.shape, one.dtype) for one in results]
        + [pltpu.SemaphoreType.DMA((3 + own_rows,))] * 2,
        compiler_params=pltpu.CompilerParams(vmem_limit_bytes=60 * 1024 * 1024),
    )(*results)
    return (mixed, cell_new, norm_new, max_new.T)


def fits_kernel(kv, tp, *args):
    tokens, w_query, cell_state, w_up = args[0], args[2], args[10], args[15]
    return (
        kv == 4
        and tp > 1
        and tokens.shape[1] % 128 == 0
        and w_query.shape[0] % 256 == 0
        and w_query.shape[1] % 256 == 0
        and args[4].shape[1] % 256 == 0
        and cell_state.shape[0] % 8 == 0
        and 2 * cell_state.shape[0] <= 128
        and cell_state.shape[3] % 128 == 0
        and w_up.shape[1] % (512 * kv) == 0
        and args[6].shape[1] <= 128
    )


def on_device(kv, tp, *args):
    if fits_kernel(kv, tp, *args):
        return fused_on_device(kv, tp, *args)
    return plain_on_device(*args)


def solution(mesh):
    in_specs = (
        P("grp", ("kv", "tp")),
        P("kv"),
        P("kv", "tp"),
        P("kv", "tp"),
        P("kv", "tp"),
        P("kv", "tp"),
        P("kv", None),
        P("kv", None),
        P(),
        P(),
        P(("grp", "kv"), "tp", None, None),
        P(("grp", "kv"), "tp", None),
        P(("grp", "kv"), "tp"),
        P("tp", "kv"),
        P("kv"),
        P("kv", "tp"),
        P("tp", "kv"),
    )
    out_specs = (
        P("grp", ("kv", "tp")),
        P(("grp", "kv"), "tp", None, None),
        P(("grp", "kv"), "tp", None),
        P(("grp", "kv"), "tp"),
    )
    return jax.shard_map(
        functools.partial(on_device, mesh.shape["kv"], mesh.shape["tp"]),
        mesh=mesh, in_specs=in_specs, out_specs=out_specs, check_vma=False
    )
```

```python
import functools

import jax
import jax.numpy as jnp
from jax import lax
from jax.experimental import pallas as pl
from jax.experimental.pallas import tpu as pltpu
from jax.sharding import PartitionSpec as P

MESH = pl.DeviceIdType.MESH
BF16 = jnp.bfloat16
F32 = jnp.float32

EPSILON = 1e-06


def memory_step(
    query, keys, values, outgate, log_input, log_forget, cell_state, norm_state, max_state
):
    max_new = jnp.maximum(log_forget + max_state, log_input)
    keep = jnp.exp(log_forget + max_state - max_new)
    write = jnp.exp(log_input - max_new)
    cell_new = (
        keep[..., None, None] * cell_state
        + (write[..., None] * keys)[..., :, None] * values[..., None, :]
    )
    norm_new = keep[..., None] * norm_state + write[..., None] * keys
    numer = jnp.einsum("shk,shkv->shv", query, cell_new, precision=lax.Precision.HIGHEST)
    denom = jnp.maximum(jnp.abs(jnp.sum(query * norm_new, axis=-1)), jnp.exp(-max_new))
    heads = (jax.nn.sigmoid(outgate) * numer / denom[..., None]).astype(jnp.bfloat16)
    return (heads, cell_new, norm_new, max_new)


def matmul(left, right):
    return jnp.dot(left, right, preferred_element_type=jnp.float32)


def plain_on_device(
    tokens,
    gain_in,
    w_query,
    w_key,
    w_value,
    w_outgate,
    w_input_gate,
    w_forget_gate,
    bias_input,
    bias_forget,
    cell_state,
    norm_state,
    max_state,
    w_proj,
    gain_mid,
    w_up,
    w_down,
):
    seq_local, head_count = (cell_state.shape[0], cell_state.shape[1])
    key_dim, value_dim = (cell_state.shape[2], cell_state.shape[3])
    head_start = lax.axis_index("tp") * head_count
    column_width = tokens.shape[1]
    D = gain_in.shape[0] * lax.axis_size("kv")
    gathered = lax.all_gather(tokens, "tp", axis=1, tiled=True)
    widef = gathered.astype(jnp.float32)
    part_squares = jnp.sum(widef * widef, axis=1)
    normed = (widef * gain_in).astype(jnp.bfloat16)
    gate_input = lax.dynamic_slice_in_dim(w_input_gate, head_start, head_count, 1)
    gate_forget = lax.dynamic_slice_in_dim(w_forget_gate, head_start, head_count, 1)
    terms = jnp.concatenate(
        [
            matmul(normed, w_query),
            matmul(normed, w_key),
            matmul(normed, w_value),
            matmul(normed, w_outgate),
            matmul(normed, gate_input),
            matmul(normed, gate_forget),
        ],
        axis=1,
    )
    total_squares = lax.psum(part_squares, "kv")
    own_terms = lax.psum_scatter(terms, "kv", scatter_dimension=0, tiled=True)
    row_squares = lax.dynamic_slice_in_dim(
        total_squares, lax.axis_index("kv") * seq_local, seq_local, 0
    )
    own_terms = own_terms * lax.rsqrt(row_squares / D + EPSILON)[:, None]
    width_qk = head_count * key_dim
    width_v = head_count * value_dim
    query = own_terms[:, :width_qk].reshape(seq_local, head_count, key_dim) * key_dim ** (-0.5)
    keys = own_terms[:, width_qk : 2 * width_qk].reshape(seq_local, head_count, key_dim)
    offset = 2 * width_qk
    values = own_terms[:, offset : offset + width_v].reshape(seq_local, head_count, value_dim)
    offset = offset + width_v
    outgate = own_terms[:, offset : offset + width_v].reshape(seq_local, head_count, value_dim)
    offset = offset + width_v
    log_input = own_terms[:, offset : offset + head_count] + lax.dynamic_slice_in_dim(
        bias_input, head_start, head_count, 0
    )
    offset = offset + head_count
    log_forget = jax.nn.log_sigmoid(
        own_terms[:, offset : offset + head_count]
        + lax.dynamic_slice_in_dim(bias_forget, head_start, head_count, 0)
    )
    heads, cell_new, norm_new, max_new = memory_step(
        query, keys, values, outgate, log_input, log_forget, cell_state, norm_state, max_state
    )
    branch_part = matmul(
        lax.all_gather(heads.reshape(seq_local, width_v), "kv", axis=0, tiled=True), w_proj
    )
    branch = lax.psum(branch_part, "tp")
    middle = (widef + branch).astype(jnp.bfloat16)
    midf = middle.astype(jnp.float32)
    mid_squares = jnp.sum(midf * midf, axis=1)
    normed_mid = (midf * gain_mid).astype(jnp.bfloat16)
    up_part = matmul(normed_mid, w_up)
    up_rows, square_rows = (
        lax.psum_scatter(up_part, "kv", scatter_dimension=0, tiled=True),
        lax.psum_scatter(mid_squares, "kv", scatter_dimension=0, tiled=True),
    )
    upward = up_rows * lax.rsqrt(square_rows / D + EPSILON)[:, None]
    hidden = jnp.square(jax.nn.relu(upward)).astype(jnp.bfloat16)
    down_part = matmul(lax.all_gather(hidden, "kv", axis=0, tiled=True), w_down)
    own_down = lax.psum_scatter(
        down_part.astype(jnp.bfloat16), "tp", scatter_dimension=1, tiled=True
    ).astype(jnp.float32)
    residual = lax.dynamic_slice_in_dim(midf, lax.axis_index("tp") * column_width, column_width, 1)
    mixed = (residual + own_down).astype(jnp.bfloat16)
    return (mixed, cell_new, norm_new, max_new)


def matmul_nt(left, right):
    return lax.dot_general(left, right, (((1,), (1,)), ((), ())), preferred_element_type=F32)


class Exchange:
    def __init__(self, sems):
        self.send_sem, self.recv_sem = sems
        self.used = 0
        self.started = []

    def copy(self, axis, target, src, dst, when=None):
        index = self.used
        self.used += 1
        one = pltpu.make_async_remote_copy(
            src_ref=src,
            dst_ref=dst,
            send_sem=self.send_sem.at[index],
            recv_sem=self.recv_sem.at[index],
            device_id={axis: target},
            device_id_type=MESH,
        )
        if when is None:
            one.start()
        else:
            pl.when(when)(one.start)
        self.started.append(one)
        return one


def partners(me, count):
    if count == 4:
        both = [3 - me, lax.rem(me + 2, 4), me + 1 - 2 * lax.rem(me, 2)]
        return both, both
    ahead = [lax.rem(me + o, count) for o in range(1, count)]
    behind = [lax.rem(me + count - o, count) for o in range(1, count)]
    return ahead, behind


def count_copies(kv, tp, subs):
    return 3 * (tp - 1) + 5 * (kv - 1) + 2 * subs * (kv - 1)


def layer_kernel(
    kv,
    tp,
    subs,
    tokens,
    gain_in,
    w_query,
    w_key,
    w_value,
    w_outgate,
    w_input_gate,
    w_forget_gate,
    bias_input,
    bias_forget,
    cell_state,
    norm_state,
    max_state,
    w_proj,
    gain_mid,
    w_up,
    w_down,
    out_v,
    cell_o,
    norm_o,
    max_o,
    tok,
    gain1,
    wqkv,
    wgi,
    wgf,
    bi,
    bf,
    cell,
    norm,
    mstate,
    wproj,
    gain2,
    wup,
    wdown,
    terms,
    b_send,
    b_recv,
    g_send,
    g_recv,
    numer,
    h_all,
    e_all,
    sq_all,
    mid,
    nmid,
    f_own,
    f_send,
    f_recv,
    hid,
    down,
    d_send,
    d_recv,
    in_sem,
    send_sem,
    recv_sem,
):
    k_me, t_me = lax.axis_index("kv"), lax.axis_index("tp")
    link = Exchange((send_sem, recv_sem))
    rows, width = tok.shape[1], tok.shape[2]
    own_rows, n_heads, key_dim, value_dim = cell.shape
    wide = tp * width
    total_width = kv * wide
    w_qk, w_v = n_heads * key_dim, n_heads * value_dim
    half = f_own.shape[2]
    block = subs * half

    loads = []

    def load(src, dst):
        one = pltpu.make_async_copy(src, dst, in_sem.at[len(loads)])
        one.start()
        loads.append(one)
        return one

    l_tok = load(tokens, tok.at[t_me])
    l_gain = load(gain_in, gain1)
    l_q = load(w_query, wqkv.at[:, 0:w_qk])
    l_k = load(w_key, wqkv.at[:, w_qk : 2 * w_qk])
    l_v = load(w_value, wqkv.at[:, 2 * w_qk : 2 * w_qk + w_v])
    l_o = load(w_outgate, wqkv.at[:, 2 * w_qk + w_v : 2 * w_qk + 2 * w_v])
    l_gates = [load(w_input_gate, wgi), load(w_forget_gate, wgf)]
    l_small = [
        load(bias_input, bi),
        load(bias_forget, bf),
        load(norm_state, norm),
        load(max_state, mstate),
    ]

    barrier = pltpu.get_barrier_semaphore()
    k_peers, k_from = partners(k_me, kv)
    t_peers, t_from = partners(t_me, tp)
    for peer in t_peers:
        pl.semaphore_signal(barrier, inc=1, device_id={"tp": peer}, device_id_type=MESH)
    for peer in k_peers:
        pl.semaphore_signal(barrier, inc=1, device_id={"kv": peer}, device_id_type=MESH)
    g_send[...] = jnp.zeros_like(g_send)
    l_tok.wait()
    pl.semaphore_wait(barrier, kv + tp - 2)

    a_copies = [link.copy("tp", p, tok.at[t_me], tok.at[t_me]) for p in t_peers]
    l_cell = load(cell_state, cell)
    l_proj = load(w_proj, wproj)
    l_gain2 = load(gain_mid, gain2)
    l_up = load(w_up, wup)
    l_down = [
        load(w_down.at[pl.ds(i * block, block)], wdown.at[pl.ds(i * block, block)])
        for i in range(kv)
    ]
    l_gain.wait()
    for one in a_copies:
        one.wait_recv()
    wide_f = jnp.concatenate([tok[i] for i in range(tp)], axis=1).astype(F32)
    squares = jnp.sum(wide_f * wide_f, axis=1, keepdims=True)
    normed = (wide_f * gain1[...]).astype(BF16)

    for one in l_gates:
        one.wait()
    n_gates = wgi.shape[0]
    shape_g = (kv, own_rows, n_gates)
    g_send[:, :, 0:n_gates] = matmul_nt(normed, wgi[...]).reshape(shape_g)
    g_send[:, :, 128 : 128 + n_gates] = matmul_nt(normed, wgf[...]).reshape(shape_g)
    g_send[:, :, 256:384] = jnp.broadcast_to(squares, (rows, 128)).reshape(kv, own_rows, 128)
    g_copies = [
        link.copy("kv", p, g_send.at[p], g_recv.at[o]) for o, p in enumerate(k_peers)
    ]
    for one in (l_q, l_k, l_v, l_o):
        one.wait()
    tile = 256

    def project(i, carry):
        cols = pl.ds(pl.multiple_of(i * tile, tile), tile)
        part = matmul(normed, wqkv[:, cols]).reshape(kv, own_rows, tile)
        terms[:, :, cols] = part
        b_send[:, :, cols] = part.astype(BF16)
        return carry

    n_tiles = wqkv.shape[1] // tile
    b_copies = []
    for low, high in ((0, n_tiles // 2), (n_tiles // 2, n_tiles)):
        lax.fori_loop(low, high, project, 0)
        cols = pl.ds(low * tile, (high - low) * tile)
        for o, p in enumerate(k_peers):
            here = b_send.at[p, :, cols], b_recv.at[o, :, cols]
            b_copies.append(link.copy("kv", p, *here))

    for one in l_small:
        one.wait()
    l_cell.wait()
    for one in g_copies:
        one.wait_recv()
    gates = g_send[k_me]
    for o in range(kv - 1):
        gates = gates + g_recv[o]
    scale = lax.rsqrt(gates[:, 256:257] / total_width + EPSILON)
    log_i = gates[:, 0:n_gates] * scale + bi[...]
    raw_f = gates[:, 128 : 128 + n_gates] * scale + bf[...]
    log_f = jnp.minimum(raw_f, 0.0) - jnp.log1p(jnp.exp(-jnp.abs(raw_f)))
    gate_lane = lax.broadcasted_iota(jnp.int32, (own_rows, n_gates), 1)
    keep, write, floor = [], [], []
    max_cols = []
    old_max = mstate[...].T
    for h in range(n_heads):
        pick = gate_lane == t_me * n_heads + h
        li = jnp.sum(jnp.where(pick, log_i, 0.0), axis=1, keepdims=True)
        lf = jnp.sum(jnp.where(pick, log_f, 0.0), axis=1, keepdims=True)
        old = old_max[:, h : h + 1]
        new = jnp.maximum(lf + old, li)
        max_cols.append(new)
        keep.append(jnp.exp(lf + old - new))
        write.append(jnp.exp(li - new))
        floor.append(jnp.exp(-new))
    head_lane = lax.broadcasted_iota(jnp.int32, (own_rows, n_heads), 1)
    new_max = jnp.broadcast_to(max_cols[0], (own_rows, n_heads))
    for h in range(1, n_heads):
        new_max = jnp.where(head_lane == h, max_cols[h], new_max)
    max_o[...] = new_max.T
    for one in b_copies:
        one.wait_recv()
    own = terms[k_me]
    for o in range(kv - 1):
        own = own + b_recv[o].astype(F32)
    own = own * scale
    query = own[:, 0:w_qk] * key_dim ** (-0.5)
    keys = own[:, w_qk : 2 * w_qk]
    values = own[:, 2 * w_qk : 2 * w_qk + w_v]
    outgate = own[:, 2 * w_qk + w_v : 2 * w_qk + 2 * w_v]
    qk_head = lax.broadcasted_iota(jnp.int32, (own_rows, w_qk), 1) // key_dim
    spread = jnp.broadcast_to(write[0], (own_rows, w_qk))
    for h in range(1, n_heads):
        spread = jnp.where(qk_head == h, write[h], spread)
    wkeys = keys * spread
    pad = jnp.zeros((128 - 2 * own_rows, w_qk), F32)
    turned = jnp.concatenate([wkeys, query, pad], axis=0).T
    denom, cross = [], []
    for h in range(n_heads):
        part = slice(h * key_dim, (h + 1) * key_dim)
        fresh = keep[h] * norm[:, h, :] + wkeys[:, part]
        norm_o[:, h, :] = fresh
        dot = jnp.sum(query[:, part] * fresh, axis=1, keepdims=True)
        shape_v = (own_rows, value_dim)
        denom.append(jnp.broadcast_to(jnp.maximum(jnp.abs(dot), floor[h]), shape_v))
        dot = jnp.sum(query[:, part] * wkeys[:, part], axis=1, keepdims=True)
        cross.append(jnp.broadcast_to(dot, shape_v))
    for h in range(n_heads):
        part = slice(h * key_dim, (h + 1) * key_dim)
        vals = slice(h * value_dim, (h + 1) * value_dim)
        for s in range(own_rows):
            q_col = turned[part, own_rows + s : own_rows + s + 1]
            numer[s : s + 1, vals] = jnp.sum(q_col * cell[s, h], axis=0, keepdims=True)
    keep_v = jnp.concatenate(
        [jnp.broadcast_to(one, (own_rows, value_dim)) for one in keep], axis=1
    )
    above = keep_v * numer[...] + jnp.concatenate(cross, axis=1) * values
    heads = jax.nn.sigmoid(outgate) * above / jnp.concatenate(denom, axis=1)
    h_all[k_me] = heads.astype(BF16)
    h_copies = [link.copy("kv", p, h_all.at[k_me], h_all.at[k_me]) for p in k_peers]
    for h in range(n_heads):
        part = slice(h * key_dim, (h + 1) * key_dim)
        vals = slice(h * value_dim, (h + 1) * value_dim)
        for s in range(own_rows):
            cell_o[s, h] = (
                keep[h][s : s + 1, :] * cell[s, h]
                + turned[part, s : s + 1] * values[s : s + 1, vals]
            )
    l_proj.wait()
    for one in h_copies:
        one.wait_recv()
    all_heads = jnp.concatenate([h_all[i].astype(F32) for i in range(kv)], axis=0)

    e_all[t_me] = matmul(all_heads.astype(BF16), wproj[...]).astype(BF16)
    e_copies = [link.copy("tp", p, e_all.at[t_me], e_all.at[t_me]) for p in t_peers]
    l_gain2.wait()
    for one in e_copies:
        one.wait_recv()
    branch = e_all[0].astype(F32)
    for i in range(1, tp):
        branch = branch + e_all[i].astype(F32)
    wide_f = jnp.concatenate([tok[i] for i in range(tp)], axis=1).astype(F32)
    middle = (wide_f + branch).astype(BF16).astype(F32)
    for i in range(tp):
        mid[i] = middle[:, i * width : (i + 1) * width]
    sq_all[k_me] = jnp.broadcast_to(jnp.sum(middle * middle, axis=1, keepdims=True), (rows, 128))
    s_copies = [link.copy("kv", p, sq_all.at[k_me], sq_all.at[k_me]) for p in k_peers]
    nmid[...] = (middle * gain2[...]).astype(BF16)

    l_up.wait()
    f_copies = {}

    def raise_block(target, sub, put):
        first = target * block + sub * half

        def raise_tile(i, carry):
            cols = pl.ds(pl.multiple_of(first + i * tile, tile), tile)
            put(pl.ds(pl.multiple_of(i * tile, tile), tile), matmul(nmid[...], wup[:, cols]))
            return carry

        lax.fori_loop(0, half // tile, raise_tile, 0)

    is_end = jnp.logical_or(k_me == 0, k_me == kv - 1)
    is_mid = jnp.logical_not(is_end)
    across, skip, near = k_peers
    targets = [across, jnp.where(is_end, near, skip), near]
    for o in (1, 0, 2):
        for sub in range(subs):

            def put_sent(here, part, o=o, sub=sub):
                f_send[o, sub, :, here] = part.astype(BF16)

            raise_block(k_peers[o], sub, put_sent)
            f_copies[o, sub] = link.copy(
                "kv",
                targets[o],
                f_send.at[o, sub],
                f_recv.at[o, sub],
                when=None if o else is_end,
            )
    for sub in range(subs):
        f_copies[1, sub].wait_recv()

        def relay(sub=sub):
            both = f_send[0, sub].astype(F32) + f_recv[1, sub].astype(F32)
            f_send[0, sub] = both.astype(BF16)
            f_copies[0, sub].start()

        pl.when(is_mid)(relay)

        def put_own(here, part, sub=sub):
            f_own[sub, :, here] = part

        raise_block(k_me, sub, put_own)
    for one in s_copies:
        one.wait_recv()
    row_sum = sq_all[0, :, 0:1]
    for i in range(1, kv):
        row_sum = row_sum + sq_all[i, :, 0:1]
    scale_mid = lax.rsqrt(row_sum / total_width + EPSILON)
    g2_copies = {}
    for sub in range(subs):
        upward = f_own[sub]
        f_copies[0, sub].wait_recv()
        f_copies[2, sub].wait_recv()
        skipped = jnp.where(is_end, f_recv[1, sub].astype(F32), 0.0)
        upward = upward + f_recv[0, sub].astype(F32) + skipped + f_recv[2, sub].astype(F32)
        hid[k_me, sub] = jnp.square(jnp.maximum(upward * scale_mid, 0.0)).astype(BF16)
        mine = hid.at[k_me, sub]
        for o, peer in enumerate(k_peers):
            g2_copies[o, sub] = link.copy("kv", peer, mine, mine)

    for one in l_down:
        one.wait()

    def lower_block(source, sub, first):
        deep = pl.ds(pl.multiple_of(source * block + sub * half, half), half)
        part = matmul(hid[source, sub], wdown[deep, :])
        down[...] = part if first else down[...] + part

    for sub in range(subs):
        lower_block(k_me, sub, sub == 0)
    for sub in range(subs):
        for o in (2, 1, 0):
            g2_copies[o, sub].wait_recv()
            lower_block(k_from[o], sub, False)
    for i in range(tp):
        d_send[i] = down[:, i * width : (i + 1) * width].astype(BF16)
    d_copies = [
        link.copy("tp", p, d_send.at[p], d_recv.at[o]) for o, p in enumerate(t_peers)
    ]
    lower = d_send[t_me].astype(F32)
    for o, one in enumerate(d_copies):
        one.wait_recv()
        lower = lower + d_recv[o].astype(F32)
    out_v[...] = (mid[t_me] + lower).astype(BF16)
    for one in link.started:
        one.wait_send()


def finish_kernel(*refs):
    sources, outs, sem = refs[0:4], refs[4:8], refs[8]
    copies = [pltpu.make_async_copy(sources[i], outs[i], sem.at[i]) for i in range(4)]
    for one in copies:
        one.start()
    for one in copies:
        one.wait()


def fused_on_device(kv, tp, *args):
    (tokens, gain_in, w_query, w_key, w_value, w_outgate, w_input_gate, w_forget_gate) = args[:8]
    (bias_input, bias_forget, cell_state, norm_state, max_state) = args[8:13]
    (w_proj, gain_mid, w_up, w_down) = args[13:]
    rows, width = tokens.shape
    own_rows = cell_state.shape[0]
    wide = w_query.shape[0]
    n_qkv = w_query.shape[1] + w_key.shape[1] + w_value.shape[1] + w_outgate.shape[1]
    hidden = w_up.shape[1]
    subs = 4 if hidden % (1024 * kv) == 0 else 2
    half = hidden // (kv * subs)
    w_v = w_value.shape[1]
    operands = tuple(pltpu.with_memory_space_constraint(x, pltpu.HBM) for x in (
        tokens,
        gain_in.reshape(1, -1),
        w_query,
        w_key,
        w_value,
        w_outgate,
        w_input_gate.T,
        w_forget_gate.T,
        bias_input.reshape(1, -1),
        bias_forget.reshape(1, -1),
        cell_state,
        norm_state,
        max_state.T,
        w_proj,
        gain_mid.reshape(1, -1),
        w_up,
        w_down,
    ))
    n_copies = count_copies(kv, tp, subs)
    vm = pltpu.VMEM
    scratch = [
        vm((tp, rows, width), BF16),
        vm((1, wide), F32),
        vm((wide, n_qkv), BF16),
        vm(w_input_gate.shape[::-1], BF16),
        vm(w_forget_gate.shape[::-1], BF16),
        vm((1, bias_input.shape[0]), F32),
        vm((1, bias_forget.shape[0]), F32),
        vm(cell_state.shape, F32),
        vm(norm_state.shape, F32),
        vm(max_state.shape[::-1], F32),
        vm(w_proj.shape, BF16),
        vm((1, wide), F32),
        vm(w_up.shape, BF16),
        vm(w_down.shape, BF16),
        vm((kv, own_rows, n_qkv), F32),
        vm((kv, own_rows, n_qkv), BF16),
        vm((kv - 1, own_rows, n_qkv), BF16),
        vm((kv, own_rows, 384), F32),
        vm((kv - 1, own_rows, 384), F32),
        vm((own_rows, w_v), F32),
        vm((kv, own_rows, w_v), BF16),
        vm((tp, rows, wide), BF16),
        vm((kv, rows, 128), F32),
        vm((tp, rows, width), F32),
        vm((rows, wide), BF16),
        vm((subs, rows, half), F32),
        vm((kv - 1, subs, rows, half), BF16),
        vm((kv - 1, subs, rows, half), BF16),
        vm((kv, subs, rows, half), BF16),
        vm((rows, wide), F32),
        vm((tp, rows, width), BF16),
        vm((tp - 1, rows, width), BF16),
        pltpu.SemaphoreType.DMA((16 + kv,)),
        pltpu.SemaphoreType.DMA((n_copies,)),
        pltpu.SemaphoreType.DMA((n_copies,)),
    ]
    anywhere = pl.BlockSpec(memory_space=pltpu.HBM)
    in_vmem = pl.BlockSpec(memory_space=pltpu.VMEM)
    results = pl.pallas_call(
        functools.partial(layer_kernel, kv, tp, subs),
        out_shape=(
            jax.ShapeDtypeStruct((rows, width), BF16),
            jax.ShapeDtypeStruct(cell_state.shape, F32),
            jax.ShapeDtypeStruct(norm_state.shape, F32),
            jax.ShapeDtypeStruct(max_state.shape[::-1], F32),
        ),
        in_specs=[anywhere] * len(operands),
        out_specs=(in_vmem,) * 4,
        scratch_shapes=scratch,
        compiler_params=pltpu.CompilerParams(
            collective_id=0, has_side_effects=True, vmem_limit_bytes=36 * 1024 * 1024
        ),
    )(*operands)
    mixed, cell_new, norm_new, max_new = pl.pallas_call(
        finish_kernel,
        out_shape=tuple(jax.ShapeDtypeStruct(one.shape, one.dtype) for one in results),
        in_specs=[in_vmem] * 4,
        out_specs=(anywhere,) * 4,
        scratch_shapes=[pltpu.SemaphoreType.DMA((4,))],
        compiler_params=pltpu.CompilerParams(vmem_limit_bytes=8 * 1024 * 1024),
    )(*results)
    return (mixed, cell_new, norm_new, max_new.T)


def fits_kernel(kv, tp, *args):
    tokens, w_query, cell_state, w_up = args[0], args[2], args[10], args[15]
    return (
        kv == 4
        and tp > 1
        and tokens.shape[1] % 128 == 0
        and w_query.shape[0] % 256 == 0
        and w_query.shape[1] % 256 == 0
        and args[4].shape[1] % 256 == 0
        and cell_state.shape[0] % 8 == 0
        and 2 * cell_state.shape[0] <= 128
        and cell_state.shape[3] % 128 == 0
        and w_up.shape[1] % (512 * kv) == 0
        and args[6].shape[1] <= 128
    )


def on_device(kv, tp, *args):
    if fits_kernel(kv, tp, *args):
        return fused_on_device(kv, tp, *args)
    return plain_on_device(*args)


def solution(mesh):
    in_specs = (
        P("grp", ("kv", "tp")),
        P("kv"),
        P("kv", "tp"),
        P("kv", "tp"),
        P("kv", "tp"),
        P("kv", "tp"),
        P("kv", None),
        P("kv", None),
        P(),
        P(),
        P(("grp", "kv"), "tp", None, None),
        P(("grp", "kv"), "tp", None),
        P(("grp", "kv"), "tp"),
        P("tp", "kv"),
        P("kv"),
        P("kv", "tp"),
        P("tp", "kv"),
    )
    out_specs = (
        P("grp", ("kv", "tp")),
        P(("grp", "kv"), "tp", None, None),
        P(("grp", "kv"), "tp", None),
        P(("grp", "kv"), "tp"),
    )
    return jax.shard_map(
        functools.partial(on_device, mesh.shape["kv"], mesh.shape["tp"]),
        mesh=mesh, in_specs=in_specs, out_specs=out_specs, check_vma=False
    )
```

```python
import functools

import jax
import jax.numpy as jnp
from jax import lax
from jax.experimental import pallas as pl
from jax.experimental.pallas import tpu as pltpu
from jax.sharding import PartitionSpec as P

MESH = pl.DeviceIdType.MESH
BF16 = jnp.bfloat16
F32 = jnp.float32

EPSILON = 1e-06


def memory_step(
    query, keys, values, outgate, log_input, log_forget, cell_state, norm_state, max_state
):
    max_new = jnp.maximum(log_forget + max_state, log_input)
    keep = jnp.exp(log_forget + max_state - max_new)
    write = jnp.exp(log_input - max_new)
    cell_new = (
        keep[..., None, None] * cell_state
        + (write[..., None] * keys)[..., :, None] * values[..., None, :]
    )
    norm_new = keep[..., None] * norm_state + write[..., None] * keys
    numer = jnp.einsum("shk,shkv->shv", query, cell_new, precision=lax.Precision.HIGHEST)
    denom = jnp.maximum(jnp.abs(jnp.sum(query * norm_new, axis=-1)), jnp.exp(-max_new))
    heads = (jax.nn.sigmoid(outgate) * numer / denom[..., None]).astype(jnp.bfloat16)
    return (heads, cell_new, norm_new, max_new)


def matmul(left, right):
    return jnp.dot(left, right, preferred_element_type=jnp.float32)


def plain_on_device(
    tokens,
    gain_in,
    w_query,
    w_key,
    w_value,
    w_outgate,
    w_input_gate,
    w_forget_gate,
    bias_input,
    bias_forget,
    cell_state,
    norm_state,
    max_state,
    w_proj,
    gain_mid,
    w_up,
    w_down,
):
    seq_local, head_count = (cell_state.shape[0], cell_state.shape[1])
    key_dim, value_dim = (cell_state.shape[2], cell_state.shape[3])
    head_start = lax.axis_index("tp") * head_count
    column_width = tokens.shape[1]
    D = gain_in.shape[0] * lax.axis_size("kv")
    gathered = lax.all_gather(tokens, "tp", axis=1, tiled=True)
    widef = gathered.astype(jnp.float32)
    part_squares = jnp.sum(widef * widef, axis=1)
    normed = (widef * gain_in).astype(jnp.bfloat16)
    gate_input = lax.dynamic_slice_in_dim(w_input_gate, head_start, head_count, 1)
    gate_forget = lax.dynamic_slice_in_dim(w_forget_gate, head_start, head_count, 1)
    terms = jnp.concatenate(
        [
            matmul(normed, w_query),
            matmul(normed, w_key),
            matmul(normed, w_value),
            matmul(normed, w_outgate),
            matmul(normed, gate_input),
            matmul(normed, gate_forget),
        ],
        axis=1,
    )
    total_squares = lax.psum(part_squares, "kv")
    own_terms = lax.psum_scatter(terms, "kv", scatter_dimension=0, tiled=True)
    row_squares = lax.dynamic_slice_in_dim(
        total_squares, lax.axis_index("kv") * seq_local, seq_local, 0
    )
    own_terms = own_terms * lax.rsqrt(row_squares / D + EPSILON)[:, None]
    width_qk = head_count * key_dim
    width_v = head_count * value_dim
    query = own_terms[:, :width_qk].reshape(seq_local, head_count, key_dim) * key_dim ** (-0.5)
    keys = own_terms[:, width_qk : 2 * width_qk].reshape(seq_local, head_count, key_dim)
    offset = 2 * width_qk
    values = own_terms[:, offset : offset + width_v].reshape(seq_local, head_count, value_dim)
    offset = offset + width_v
    outgate = own_terms[:, offset : offset + width_v].reshape(seq_local, head_count, value_dim)
    offset = offset + width_v
    log_input = own_terms[:, offset : offset + head_count] + lax.dynamic_slice_in_dim(
        bias_input, head_start, head_count, 0
    )
    offset = offset + head_count
    log_forget = jax.nn.log_sigmoid(
        own_terms[:, offset : offset + head_count]
        + lax.dynamic_slice_in_dim(bias_forget, head_start, head_count, 0)
    )
    heads, cell_new, norm_new, max_new = memory_step(
        query, keys, values, outgate, log_input, log_forget, cell_state, norm_state, max_state
    )
    branch_part = matmul(
        lax.all_gather(heads.reshape(seq_local, width_v), "kv", axis=0, tiled=True), w_proj
    )
    branch = lax.psum(branch_part, "tp")
    middle = (widef + branch).astype(jnp.bfloat16)
    midf = middle.astype(jnp.float32)
    mid_squares = jnp.sum(midf * midf, axis=1)
    normed_mid = (midf * gain_mid).astype(jnp.bfloat16)
    up_part = matmul(normed_mid, w_up)
    up_rows, square_rows = (
        lax.psum_scatter(up_part, "kv", scatter_dimension=0, tiled=True),
        lax.psum_scatter(mid_squares, "kv", scatter_dimension=0, tiled=True),
    )
    upward = up_rows * lax.rsqrt(square_rows / D + EPSILON)[:, None]
    hidden = jnp.square(jax.nn.relu(upward)).astype(jnp.bfloat16)
    down_part = matmul(lax.all_gather(hidden, "kv", axis=0, tiled=True), w_down)
    own_down = lax.psum_scatter(
        down_part.astype(jnp.bfloat16), "tp", scatter_dimension=1, tiled=True
    ).astype(jnp.float32)
    residual = lax.dynamic_slice_in_dim(midf, lax.axis_index("tp") * column_width, column_width, 1)
    mixed = (residual + own_down).astype(jnp.bfloat16)
    return (mixed, cell_new, norm_new, max_new)


def matmul_nt(left, right):
    return lax.dot_general(left, right, (((1,), (1,)), ((), ())), preferred_element_type=F32)


class Exchange:
    def __init__(self, sems):
        self.send_sem, self.recv_sem = sems
        self.used = 0
        self.started = []

    def copy(self, axis, target, src, dst, when=None):
        index = self.used
        self.used += 1
        one = pltpu.make_async_remote_copy(
            src_ref=src,
            dst_ref=dst,
            send_sem=self.send_sem.at[index],
            recv_sem=self.recv_sem.at[index],
            device_id={axis: target},
            device_id_type=MESH,
        )
        if when is None:
            one.start()
        else:
            pl.when(when)(one.start)
        self.started.append(one)
        return one


def partners(me, count):
    if count == 4:
        both = [3 - me, lax.rem(me + 2, 4), me + 1 - 2 * lax.rem(me, 2)]
        return both, both
    ahead = [lax.rem(me + o, count) for o in range(1, count)]
    behind = [lax.rem(me + count - o, count) for o in range(1, count)]
    return ahead, behind


def count_copies(kv, tp, subs):
    return 3 * (tp - 1) + 5 * (kv - 1) + 2 * subs * (kv - 1)


def layer_kernel(
    kv,
    tp,
    subs,
    tokens,
    gain_in,
    w_query,
    w_key,
    w_value,
    w_outgate,
    w_input_gate,
    w_forget_gate,
    bias_input,
    bias_forget,
    cell_state,
    norm_state,
    max_state,
    w_proj,
    gain_mid,
    w_up,
    w_down,
    out_v,
    cell_o,
    norm_o,
    max_o,
    tok,
    gain1,
    wqkv,
    wgi,
    wgf,
    bi,
    bf,
    cell,
    norm,
    mstate,
    wproj,
    gain2,
    wup,
    wdown,
    terms,
    b_send,
    b_recv,
    g_send,
    g_recv,
    numer,
    h_all,
    e_all,
    sq_all,
    mid,
    nmid,
    f_own,
    f_send,
    f_recv,
    hid,
    down,
    d_send,
    d_recv,
    in_sem,
    send_sem,
    recv_sem,
):
    k_me, t_me = lax.axis_index("kv"), lax.axis_index("tp")
    link = Exchange((send_sem, recv_sem))
    rows, width = tok.shape[1], tok.shape[2]
    own_rows, n_heads, key_dim, value_dim = cell.shape
    wide = tp * width
    total_width = kv * wide
    w_qk, w_v = n_heads * key_dim, n_heads * value_dim
    half = f_own.shape[2]
    block = subs * half

    loads = []

    def load(src, dst):
        one = pltpu.make_async_copy(src, dst, in_sem.at[len(loads)])
        one.start()
        loads.append(one)
        return one

    l_tok = load(tokens, tok.at[t_me])
    l_gain = load(gain_in, gain1)
    l_q = load(w_query, wqkv.at[:, 0:w_qk])
    l_k = load(w_key, wqkv.at[:, w_qk : 2 * w_qk])
    l_v = load(w_value, wqkv.at[:, 2 * w_qk : 2 * w_qk + w_v])
    l_o = load(w_outgate, wqkv.at[:, 2 * w_qk + w_v : 2 * w_qk + 2 * w_v])
    l_gates = [load(w_input_gate, wgi), load(w_forget_gate, wgf)]
    l_small = [
        load(bias_input, bi),
        load(bias_forget, bf),
        load(norm_state, norm),
        load(max_state, mstate),
    ]

    barrier = pltpu.get_barrier_semaphore()
    k_peers, k_from = partners(k_me, kv)
    t_peers, t_from = partners(t_me, tp)
    for peer in t_peers:
        pl.semaphore_signal(barrier, inc=1, device_id={"tp": peer}, device_id_type=MESH)
    for peer in k_peers:
        pl.semaphore_signal(barrier, inc=1, device_id={"kv": peer}, device_id_type=MESH)
    g_send[...] = jnp.zeros_like(g_send)
    l_tok.wait()
    pl.semaphore_wait(barrier, kv + tp - 2)

    a_copies = [link.copy("tp", p, tok.at[t_me], tok.at[t_me]) for p in t_peers]
    l_cell = load(cell_state, cell)
    l_proj = load(w_proj, wproj)
    l_gain2 = load(gain_mid, gain2)
    l_up = load(w_up, wup)
    l_down = [
        load(w_down.at[pl.ds(i * block, block)], wdown.at[pl.ds(i * block, block)])
        for i in range(kv)
    ]
    l_gain.wait()
    for one in a_copies:
        one.wait_recv()
    wide_f = jnp.concatenate([tok[i] for i in range(tp)], axis=1).astype(F32)
    squares = jnp.sum(wide_f * wide_f, axis=1, keepdims=True)
    normed = (wide_f * gain1[...]).astype(BF16)

    for one in l_gates:
        one.wait()
    n_gates = wgi.shape[0]
    shape_g = (kv, own_rows, n_gates)
    g_send[:, :, 0:n_gates] = matmul_nt(normed, wgi[...]).reshape(shape_g)
    g_send[:, :, 128 : 128 + n_gates] = matmul_nt(normed, wgf[...]).reshape(shape_g)
    g_send[:, :, 256:384] = jnp.broadcast_to(squares, (rows, 128)).reshape(kv, own_rows, 128)
    g_copies = [
        link.copy("kv", p, g_send.at[p], g_recv.at[o]) for o, p in enumerate(k_peers)
    ]
    for one in (l_q, l_k, l_v, l_o):
        one.wait()
    n_qkv = wqkv.shape[1]
    b_copies = []
    for low, high in ((0, n_qkv // 2), (n_qkv // 2, n_qkv)):
        part = matmul(normed, wqkv[:, low:high]).reshape(kv, own_rows, high - low)
        terms[:, :, low:high] = part
        b_send[:, :, low:high] = part.astype(BF16)
        cols = pl.ds(low, high - low)
        for o, p in enumerate(k_peers):
            here = b_send.at[p, :, cols], b_recv.at[o, :, cols]
            b_copies.append(link.copy("kv", p, *here))

    for one in l_small:
        one.wait()
    l_cell.wait()
    for one in g_copies:
        one.wait_recv()
    gates = g_send[k_me]
    for o in range(kv - 1):
        gates = gates + g_recv[o]
    scale = lax.rsqrt(gates[:, 256:257] / total_width + EPSILON)
    log_i = gates[:, 0:n_gates] * scale + bi[...]
    raw_f = gates[:, 128 : 128 + n_gates] * scale + bf[...]
    log_f = jnp.minimum(raw_f, 0.0) - jnp.log1p(jnp.exp(-jnp.abs(raw_f)))
    gate_lane = lax.broadcasted_iota(jnp.int32, (own_rows, n_gates), 1)
    keep, write, floor = [], [], []
    max_cols = []
    old_max = mstate[...].T
    for h in range(n_heads):
        pick = gate_lane == t_me * n_heads + h
        li = jnp.sum(jnp.where(pick, log_i, 0.0), axis=1, keepdims=True)
        lf = jnp.sum(jnp.where(pick, log_f, 0.0), axis=1, keepdims=True)
        old = old_max[:, h : h + 1]
        new = jnp.maximum(lf + old, li)
        max_cols.append(new)
        keep.append(jnp.exp(lf + old - new))
        write.append(jnp.exp(li - new))
        floor.append(jnp.exp(-new))
    head_lane = lax.broadcasted_iota(jnp.int32, (own_rows, n_heads), 1)
    new_max = jnp.broadcast_to(max_cols[0], (own_rows, n_heads))
    for h in range(1, n_heads):
        new_max = jnp.where(head_lane == h, max_cols[h], new_max)
    max_o[...] = new_max.T
    for one in b_copies:
        one.wait_recv()
    own = terms[k_me]
    for o in range(kv - 1):
        own = own + b_recv[o].astype(F32)
    own = own * scale
    query = own[:, 0:w_qk] * key_dim ** (-0.5)
    keys = own[:, w_qk : 2 * w_qk]
    values = own[:, 2 * w_qk : 2 * w_qk + w_v]
    outgate = own[:, 2 * w_qk + w_v : 2 * w_qk + 2 * w_v]
    qk_head = lax.broadcasted_iota(jnp.int32, (own_rows, w_qk), 1) // key_dim
    spread = jnp.broadcast_to(write[0], (own_rows, w_qk))
    for h in range(1, n_heads):
        spread = jnp.where(qk_head == h, write[h], spread)
    wkeys = keys * spread
    pad = jnp.zeros((128 - 2 * own_rows, w_qk), F32)
    turned = jnp.concatenate([wkeys, query, pad], axis=0).T
    denom, cross = [], []
    for h in range(n_heads):
        part = slice(h * key_dim, (h + 1) * key_dim)
        fresh = keep[h] * norm[:, h, :] + wkeys[:, part]
        norm_o[:, h, :] = fresh
        dot = jnp.sum(query[:, part] * fresh, axis=1, keepdims=True)
        shape_v = (own_rows, value_dim)
        denom.append(jnp.broadcast_to(jnp.maximum(jnp.abs(dot), floor[h]), shape_v))
        dot = jnp.sum(query[:, part] * wkeys[:, part], axis=1, keepdims=True)
        cross.append(jnp.broadcast_to(dot, shape_v))
    for h in range(n_heads):
        part = slice(h * key_dim, (h + 1) * key_dim)
        vals = slice(h * value_dim, (h + 1) * value_dim)
        for s in range(own_rows):
            q_col = turned[part, own_rows + s : own_rows + s + 1]
            numer[s : s + 1, vals] = jnp.sum(q_col * cell[s, h], axis=0, keepdims=True)
    keep_v = jnp.concatenate(
        [jnp.broadcast_to(one, (own_rows, value_dim)) for one in keep], axis=1
    )
    above = keep_v * numer[...] + jnp.concatenate(cross, axis=1) * values
    heads = jax.nn.sigmoid(outgate) * above / jnp.concatenate(denom, axis=1)
    h_all[k_me] = heads.astype(BF16)
    h_copies = [link.copy("kv", p, h_all.at[k_me], h_all.at[k_me]) for p in k_peers]
    for h in range(n_heads):
        part = slice(h * key_dim, (h + 1) * key_dim)
        vals = slice(h * value_dim, (h + 1) * value_dim)
        for s in range(own_rows):
            cell_o[s, h] = (
                keep[h][s : s + 1, :] * cell[s, h]
                + turned[part, s : s + 1] * values[s : s + 1, vals]
            )
    l_proj.wait()
    for one in h_copies:
        one.wait_recv()
    all_heads = jnp.concatenate([h_all[i].astype(F32) for i in range(kv)], axis=0)

    e_all[t_me] = matmul(all_heads.astype(BF16), wproj[...]).astype(BF16)
    e_copies = [link.copy("tp", p, e_all.at[t_me], e_all.at[t_me]) for p in t_peers]
    l_gain2.wait()
    for one in e_copies:
        one.wait_recv()
    branch = e_all[0].astype(F32)
    for i in range(1, tp):
        branch = branch + e_all[i].astype(F32)
    wide_f = jnp.concatenate([tok[i] for i in range(tp)], axis=1).astype(F32)
    middle = (wide_f + branch).astype(BF16).astype(F32)
    for i in range(tp):
        mid[i] = middle[:, i * width : (i + 1) * width]
    sq_all[k_me] = jnp.broadcast_to(jnp.sum(middle * middle, axis=1, keepdims=True), (rows, 128))
    s_copies = [link.copy("kv", p, sq_all.at[k_me], sq_all.at[k_me]) for p in k_peers]
    nmid[...] = (middle * gain2[...]).astype(BF16)

    l_up.wait()
    f_copies = {}

    pair = 2

    def raise_block(target, sub):
        first = pl.multiple_of(target * block + sub * half, half)
        return matmul(nmid[...], wup[:, pl.ds(first, pair * half)])

    is_end = jnp.logical_or(k_me == 0, k_me == kv - 1)
    is_mid = jnp.logical_not(is_end)
    across, skip, near = k_peers
    targets = [across, jnp.where(is_end, near, skip), near]
    for o in (1, 0, 2):
        for low in range(0, subs, pair):
            part = raise_block(k_peers[o], low).astype(BF16)
            for sub in range(low, low + pair):
                f_send[o, sub] = part[:, (sub - low) * half : (sub - low + 1) * half]
                f_copies[o, sub] = link.copy(
                    "kv",
                    targets[o],
                    f_send.at[o, sub],
                    f_recv.at[o, sub],
                    when=None if o else is_end,
                )
    for sub in range(subs):
        f_copies[1, sub].wait_recv()

        def relay(sub=sub):
            both = f_send[0, sub].astype(F32) + f_recv[1, sub].astype(F32)
            f_send[0, sub] = both.astype(BF16)
            f_copies[0, sub].start()

        pl.when(is_mid)(relay)
        if sub % pair == 0:
            part = raise_block(k_me, sub)
            for i in range(pair):
                f_own[sub + i] = part[:, i * half : (i + 1) * half]
    for one in s_copies:
        one.wait_recv()
    row_sum = sq_all[0, :, 0:1]
    for i in range(1, kv):
        row_sum = row_sum + sq_all[i, :, 0:1]
    scale_mid = lax.rsqrt(row_sum / total_width + EPSILON)
    g2_copies = {}
    for sub in range(subs):
        upward = f_own[sub]
        f_copies[0, sub].wait_recv()
        f_copies[2, sub].wait_recv()
        skipped = jnp.where(is_end, f_recv[1, sub].astype(F32), 0.0)
        upward = upward + f_recv[0, sub].astype(F32) + skipped + f_recv[2, sub].astype(F32)
        hid[k_me, sub] = jnp.square(jnp.maximum(upward * scale_mid, 0.0)).astype(BF16)
        mine = hid.at[k_me, sub]
        for o, peer in enumerate(k_peers):
            g2_copies[o, sub] = link.copy("kv", peer, mine, mine)

    for one in l_down:
        one.wait()

    def lower_block(source, sub, first):
        deep = pl.ds(pl.multiple_of(source * block + sub * half, half), half)
        part = matmul(hid[source, sub], wdown[deep, :])
        down[...] = part if first else down[...] + part

    for sub in range(subs):
        lower_block(k_me, sub, sub == 0)
    for sub in range(subs):
        for o in (2, 1, 0):
            g2_copies[o, sub].wait_recv()
            lower_block(k_from[o], sub, False)
    for i in range(tp):
        d_send[i] = down[:, i * width : (i + 1) * width].astype(BF16)
    d_copies = [
        link.copy("tp", p, d_send.at[p], d_recv.at[o]) for o, p in enumerate(t_peers)
    ]
    lower = d_send[t_me].astype(F32)
    for o, one in enumerate(d_copies):
        one.wait_recv()
        lower = lower + d_recv[o].astype(F32)
    out_v[...] = (mid[t_me] + lower).astype(BF16)
    for one in link.started:
        one.wait_send()


def finish_kernel(*refs):
    sources, outs, sem = refs[0:4], refs[4:8], refs[8]
    copies = [pltpu.make_async_copy(sources[i], outs[i], sem.at[i]) for i in range(4)]
    for one in copies:
        one.start()
    for one in copies:
        one.wait()


def fused_on_device(kv, tp, *args):
    (tokens, gain_in, w_query, w_key, w_value, w_outgate, w_input_gate, w_forget_gate) = args[:8]
    (bias_input, bias_forget, cell_state, norm_state, max_state) = args[8:13]
    (w_proj, gain_mid, w_up, w_down) = args[13:]
    rows, width = tokens.shape
    own_rows = cell_state.shape[0]
    wide = w_query.shape[0]
    n_qkv = w_query.shape[1] + w_key.shape[1] + w_value.shape[1] + w_outgate.shape[1]
    hidden = w_up.shape[1]
    subs = 4 if hidden % (1024 * kv) == 0 else 2
    half = hidden // (kv * subs)
    w_v = w_value.shape[1]
    operands = tuple(pltpu.with_memory_space_constraint(x, pltpu.HBM) for x in (
        tokens,
        gain_in.reshape(1, -1),
        w_query,
        w_key,
        w_value,
        w_outgate,
        w_input_gate.T,
        w_forget_gate.T,
        bias_input.reshape(1, -1),
        bias_forget.reshape(1, -1),
        cell_state,
        norm_state,
        max_state.T,
        w_proj,
        gain_mid.reshape(1, -1),
        w_up,
        w_down,
    ))
    n_copies = count_copies(kv, tp, subs)
    vm = pltpu.VMEM
    scratch = [
        vm((tp, rows, width), BF16),
        vm((1, wide), F32),
        vm((wide, n_qkv), BF16),
        vm(w_input_gate.shape[::-1], BF16),
        vm(w_forget_gate.shape[::-1], BF16),
        vm((1, bias_input.shape[0]), F32),
        vm((1, bias_forget.shape[0]), F32),
        vm(cell_state.shape, F32),
        vm(norm_state.shape, F32),
        vm(max_state.shape[::-1], F32),
        vm(w_proj.shape, BF16),
        vm((1, wide), F32),
        vm(w_up.shape, BF16),
        vm(w_down.shape, BF16),
        vm((kv, own_rows, n_qkv), F32),
        vm((kv, own_rows, n_qkv), BF16),
        vm((kv - 1, own_rows, n_qkv), BF16),
        vm((kv, own_rows, 384), F32),
        vm((kv - 1, own_rows, 384), F32),
        vm((own_rows, w_v), F32),
        vm((kv, own_rows, w_v), BF16),
        vm((tp, rows, wide), BF16),
        vm((kv, rows, 128), F32),
        vm((tp, rows, width), F32),
        vm((rows, wide), BF16),
        vm((subs, rows, half), F32),
        vm((kv - 1, subs, rows, half), BF16),
        vm((kv - 1, subs, rows, half), BF16),
        vm((kv, subs, rows, half), BF16),
        vm((rows, wide), F32),
        vm((tp, rows, width), BF16),
        vm((tp - 1, rows, width), BF16),
        pltpu.SemaphoreType.DMA((16 + kv,)),
        pltpu.SemaphoreType.DMA((n_copies,)),
        pltpu.SemaphoreType.DMA((n_copies,)),
    ]
    anywhere = pl.BlockSpec(memory_space=pltpu.HBM)
    in_vmem = pl.BlockSpec(memory_space=pltpu.VMEM)
    results = pl.pallas_call(
        functools.partial(layer_kernel, kv, tp, subs),
        out_shape=(
            jax.ShapeDtypeStruct((rows, width), BF16),
            jax.ShapeDtypeStruct(cell_state.shape, F32),
            jax.ShapeDtypeStruct(norm_state.shape, F32),
            jax.ShapeDtypeStruct(max_state.shape[::-1], F32),
        ),
        in_specs=[anywhere] * len(operands),
        out_specs=(in_vmem,) * 4,
        scratch_shapes=scratch,
        compiler_params=pltpu.CompilerParams(
            collective_id=0, has_side_effects=True, vmem_limit_bytes=36 * 1024 * 1024
        ),
    )(*operands)
    mixed, cell_new, norm_new, max_new = pl.pallas_call(
        finish_kernel,
        out_shape=tuple(jax.ShapeDtypeStruct(one.shape, one.dtype) for one in results),
        in_specs=[in_vmem] * 4,
        out_specs=(anywhere,) * 4,
        scratch_shapes=[pltpu.SemaphoreType.DMA((4,))],
        compiler_params=pltpu.CompilerParams(vmem_limit_bytes=8 * 1024 * 1024),
    )(*results)
    return (mixed, cell_new, norm_new, max_new.T)


def fits_kernel(kv, tp, *args):
    tokens, w_query, cell_state, w_up = args[0], args[2], args[10], args[15]
    return (
        kv == 4
        and tp > 1
        and tokens.shape[1] % 128 == 0
        and w_query.shape[0] % 256 == 0
        and w_query.shape[1] % 256 == 0
        and args[4].shape[1] % 256 == 0
        and cell_state.shape[0] % 8 == 0
        and 2 * cell_state.shape[0] <= 128
        and cell_state.shape[3] % 128 == 0
        and w_up.shape[1] % (512 * kv) == 0
        and args[6].shape[1] <= 128
    )


def on_device(kv, tp, *args):
    if fits_kernel(kv, tp, *args):
        return fused_on_device(kv, tp, *args)
    return plain_on_device(*args)


def solution(mesh):
    in_specs = (
        P("grp", ("kv", "tp")),
        P("kv"),
        P("kv", "tp"),
        P("kv", "tp"),
        P("kv", "tp"),
        P("kv", "tp"),
        P("kv", None),
        P("kv", None),
        P(),
        P(),
        P(("grp", "kv"), "tp", None, None),
        P(("grp", "kv"), "tp", None),
        P(("grp", "kv"), "tp"),
        P("tp", "kv"),
        P("kv"),
        P("kv", "tp"),
        P("tp", "kv"),
    )
    out_specs = (
        P("grp", ("kv", "tp")),
        P(("grp", "kv"), "tp", None, None),
        P(("grp", "kv"), "tp", None),
        P(("grp", "kv"), "tp"),
    )
    return jax.shard_map(
        functools.partial(on_device, mesh.shape["kv"], mesh.shape["tp"]),
        mesh=mesh, in_specs=in_specs, out_specs=out_specs, check_vma=False
    )
```
